512 devices in a mesh: grp: 2 (over y), sp: 32 (over z), tp: 8 (over x, core).
Axes of the slice: x: 4, y: 2, z: 32, core: 2. Of those that a mesh axis runs over, the one named last changes fastest.
The devices are a block of a 4x8x32 slice.
Arguments:
- query_rows: bfloat16 [8192, 1024], P(('grp', 'sp'), 'tp'), parts along dimension 0, may hold values from -12 to 12
- key_rows: bfloat16 [8192, 1024], P(('grp', 'sp'), 'tp'), parts along dimension 0, may hold values from -9 to 9
- value_rows: bfloat16 [8192, 1024], P(('grp', 'sp'), 'tp'), parts along dimension 0, may hold values from -6 to 6
- key_logit: bfloat16 [8192, 8], P(('grp', 'sp'), 'tp'), parts along dimension 0, as said below
- residual: bfloat16 [8192, 2048], P(('grp', 'sp')), parts along dimension 0, may hold values from -6 to 6
- out_weight: bfloat16 [1024, 2048], P('tp'), may hold values from -0.1875 to 0.1875
- mix_gain: float32 [2048], replicated, may hold values from 0.1 to 1.9
- ffn_gain: float32 [2048], replicated, may hold values from 0.1 to 1.9
- out_gain: float32 [2048], replicated, may hold values from 0.1 to 1.9
- gate_weight: bfloat16 [2048, 5120], P('sp', 'tp'), may hold values from -0.125 to 0.125
- up_weight: bfloat16 [2048, 5120], P('sp', 'tp'), may hold values from -0.125 to 0.125
- down_weight: bfloat16 [2048, 5120], P('sp', 'tp'), may hold values from -0.078125 to 0.078125
Outputs:
- layer_out: bfloat16 [8192, 2048], P(('grp', 'sp')), parts along dimension 0
The draws below stay inside these ranges and needn't reach their ends.
There are 2 independent parts, one for each index of `grp`. The reference program is written for one: setup_inputs(seed, part) draws one part's arguments, and reference() takes and returns one part's arrays. A program takes and returns all parts, laid end to end along the dimension named above; an argument that names none is the same for every part. Nothing has to cross between parts.
Inputs may be any that keep to these rules, and one draw needn't show every extreme that they name: `key_logit`: log-odds offsets of the keys, all negative.
All inputs are finite; a program needn't handle non-finite values.
Results may differ from the reference program's by a relative error of at most 0.018.
Values may be sent and summed in bfloat16 or wider, within the bound.
A program may use at most 64 MiB of HBM per device.

```python
import math
import jax
import jax.numpy as jnp
from jax import lax

D = 2048
ATTENTION_COUNT = 8
HEAD_DIM = 128
FF = 5120
TOK_DEV = 128
SEQUENCE_LENGTH = 4096
HEAD_GROUP = 1
FF_GROUP = 640
N_SP = 32
N_TP = 8


def draw_key_logit(key, part):
    flowing_entries = jax.random.split(key, 5)
    length_log = math.log(SEQUENCE_LENGTH)
    starting_shift = jax.random.uniform(flowing_entries[0], (ATTENTION_COUNT,), jnp.float32, -7.5 - length_log, -8.5)
    tile_spacing = jax.random.uniform(flowing_entries[1], (SEQUENCE_LENGTH // TOK_DEV, ATTENTION_COUNT), jnp.float32, -0.7, 0.7)
    tile_spacing = jnp.repeat(tile_spacing, TOK_DEV, axis=0)
    gaussian_perturbation = 0.3 * jax.random.normal(flowing_entries[2], (SEQUENCE_LENGTH, ATTENTION_COUNT), jnp.float32)
    spots = jax.random.randint(flowing_entries[3], (3, ATTENTION_COUNT), 0, SEQUENCE_LENGTH)
    places = jnp.arange(SEQUENCE_LENGTH, dtype=jnp.int32)[:, None, None]
    hit_entries = jnp.any(places == spots[None, :, :], axis=1)
    sudden_entries = jax.random.uniform(flowing_entries[4], (SEQUENCE_LENGTH, ATTENTION_COUNT), jnp.float32, -1.5, -0.5)
    payload_table = jnp.where(hit_entries, sudden_entries, starting_shift[None, :] + tile_spacing + gaussian_perturbation)
    return payload_table.astype(jnp.bfloat16)


def levels(own_key, shape, cuts, low, top_value):
    level, own = 1.0, jax.random.fold_in(own_key, 6)
    for dim, shards_of in cuts:
        draws = jnp.exp(jax.random.uniform(jax.random.fold_in(own, dim), (shards_of,), jnp.float32, low / len(cuts), top_value / len(cuts)))
        level = level * jnp.repeat(draws, shape[dim] // shards_of).reshape([-1 if axis == dim else 1 for axis in range(len(shape))])
    return level


def normal_values(key, dims, spread, reach, cuts=(), kind=jnp.bfloat16):
    array = spread * jax.random.normal(key, dims, jnp.float32)
    if cuts:
        array = array * levels(key, dims, cuts, -0.22, 0.18)
    return jnp.clip(array, -reach, reach).astype(kind)


def setup_inputs(seed: int = 0, part: int = 0) -> dict:
    key_list = jax.random.split(jax.random.key(seed), 13)
    part_keys = jax.random.split(jax.random.fold_in(key_list[12], part), 13)
    return {
        "query_rows": normal_values(part_keys[0], (SEQUENCE_LENGTH, ATTENTION_COUNT * HEAD_DIM), 2.0, 12.0, ((0, 32), (1, 8))),
        "key_rows": normal_values(part_keys[1], (SEQUENCE_LENGTH, ATTENTION_COUNT * HEAD_DIM), 1.5, 9.0, ((0, 32), (1, 8))),
        "value_rows": normal_values(part_keys[2], (SEQUENCE_LENGTH, ATTENTION_COUNT * HEAD_DIM), 1.0, 6.0, ((0, 32), (1, 8))),
        "key_logit": draw_key_logit(jax.random.fold_in(jax.random.fold_in(key_list[12], part), 71), part),
        "residual": normal_values(part_keys[4], (SEQUENCE_LENGTH, D), 1.0, 6.0, ((0, 32),)),
        "out_weight": normal_values(key_list[5], (ATTENTION_COUNT * HEAD_DIM, D), (ATTENTION_COUNT * HEAD_DIM) ** -0.5, 0.1875, ((0, 8),)),
        "mix_gain": jnp.clip(1.0 + 0.18 * jax.random.normal(key_list[6], (D,), jnp.float32), 0.1, 1.9),
        "ffn_gain": jnp.clip(1.0 + 0.18 * jax.random.normal(key_list[7], (D,), jnp.float32), 0.1, 1.9),
        "out_gain": jnp.clip(1.0 + 0.18 * jax.random.normal(key_list[8], (D,), jnp.float32), 0.1, 1.9),
        "gate_weight": normal_values(key_list[9], (D, FF), D ** -0.5, 0.125, ((0, 32), (1, 8))),
        "up_weight": normal_values(key_list[10], (D, FF), D ** -0.5, 0.125, ((0, 32), (1, 8))),
        "down_weight": normal_values(key_list[11], (D, FF), FF ** -0.5, 0.078125, ((0, 32), (1, 8))),
    }


epsilon = 1e-06

def normalize(payload_table):
    return payload_table * lax.rsqrt(lax.optimization_barrier(jnp.mean(payload_table * payload_table, axis=-1, keepdims=True)) + epsilon)

def block_terms(queries, key_part, value_part, logit_part, query_block, key_block):
    scores = jnp.einsum('hqd,khd->hqk', queries.astype(jnp.float32), key_part.astype(jnp.float32)) * HEAD_DIM ** (-0.5)
    scores = scores + jnp.transpose(logit_part.astype(jnp.float32))[:, None, :]
    query_pos = query_block * TOK_DEV + jnp.arange(TOK_DEV, dtype=jnp.int32)[:, None]
    key_pos = key_block * TOK_DEV + jnp.arange(TOK_DEV, dtype=jnp.int32)[None, :]
    causal = key_pos < query_pos
    keep_log = jnp.where(causal, jax.nn.log_sigmoid(-scores), 0.0)
    totals = lax.optimization_barrier(jnp.sum(keep_log, axis=2))
    within = lax.cumsum(keep_log, axis=2, reverse=True) - keep_log
    sticks = jnp.where(causal, jnp.exp(jax.nn.log_sigmoid(scores) + within), 0.0).astype(jnp.bfloat16)
    partials = jnp.einsum('hqk,khd->hqd', sticks.astype(jnp.float32), value_part.astype(jnp.float32))
    return (totals, partials)

def reference(query_rows, key_rows, value_rows, key_logit, residual, out_weight, mix_gain, ffn_gain, out_gain, gate_weight, up_weight, down_weight):

    def one_block(query_block):
        start = (query_block * TOK_DEV).astype(jnp.int32)
        queries = lax.dynamic_slice_in_dim(query_rows, start, TOK_DEV, 0).reshape(TOK_DEV, ATTENTION_COUNT, HEAD_DIM).transpose(1, 0, 2)

        def key_terms(key_block):
            key_start = (key_block * TOK_DEV).astype(jnp.int32)
            key_part = lax.dynamic_slice_in_dim(key_rows, key_start, TOK_DEV, 0).reshape(TOK_DEV, ATTENTION_COUNT, HEAD_DIM)
            value_part = lax.dynamic_slice_in_dim(value_rows, key_start, TOK_DEV, 0).reshape(TOK_DEV, ATTENTION_COUNT, HEAD_DIM)
            logit_part = lax.dynamic_slice_in_dim(key_logit, key_start, TOK_DEV, 0)

            def compute(unused):
                return block_terms(queries, key_part, value_part, logit_part, query_block, key_block)

            def skipped(unused):
                return (jnp.zeros((ATTENTION_COUNT, TOK_DEV), jnp.float32), jnp.zeros((ATTENTION_COUNT, TOK_DEV, HEAD_DIM), jnp.float32))
            return lax.cond(key_block <= query_block, compute, skipped, 0)
        totals, partials = lax.map(key_terms, jnp.arange(N_SP, dtype=jnp.int32))
        suffix = lax.cumsum(totals, axis=0, reverse=True) - totals
        attended = jnp.einsum('bhq,bhqd->qhd', jnp.exp(suffix), partials, precision=lax.Precision.HIGHEST)
        attended = attended.reshape(TOK_DEV, ATTENTION_COUNT * HEAD_DIM).astype(jnp.bfloat16)
        head_part = jnp.einsum('qgc,gcd->gqd', attended.reshape(TOK_DEV, N_TP, HEAD_GROUP * HEAD_DIM).astype(jnp.float32), out_weight.reshape(N_TP, HEAD_GROUP * HEAD_DIM, D).astype(jnp.float32)).astype(jnp.bfloat16)
        mixed_rows = lax.optimization_barrier(jnp.sum(head_part.astype(jnp.float32), axis=0)).astype(jnp.bfloat16)
        own_residual = lax.dynamic_slice_in_dim(residual, start, TOK_DEV, 0).astype(jnp.float32)
        middle = (own_residual + mix_gain * normalize(mixed_rows.astype(jnp.float32))).astype(jnp.bfloat16)
        normed = (ffn_gain * normalize(middle.astype(jnp.float32))).astype(jnp.bfloat16)
        gate_act = jnp.dot(normed, gate_weight, preferred_element_type=jnp.float32)
        up_act = jnp.dot(normed, up_weight, preferred_element_type=jnp.float32)
        hidden = (jax.nn.silu(gate_act) * up_act).astype(jnp.bfloat16)
        unit_part = jnp.einsum('qgf,dgf->gqd', hidden.reshape(TOK_DEV, N_TP, FF_GROUP).astype(jnp.float32), down_weight.reshape(D, N_TP, FF_GROUP).astype(jnp.float32)).astype(jnp.bfloat16)
        ffn_out = lax.optimization_barrier(jnp.sum(unit_part.astype(jnp.float32), axis=0)).astype(jnp.bfloat16)
        return (middle.astype(jnp.float32) + out_gain * normalize(ffn_out.astype(jnp.float32))).astype(jnp.bfloat16)
    blocks_out = lax.map(one_block, jnp.arange(N_SP, dtype=jnp.int32))
    return blocks_out.reshape(SEQUENCE_LENGTH, D)
```

```python
import functools

import jax
import jax.numpy as jnp
from jax import lax
from jax.experimental import pallas as pl
from jax.experimental.pallas import tpu as pltpu
from jax.sharding import PartitionSpec as P

EPSILON = 1e-06
MESH = pl.DeviceIdType.MESH
F32 = jnp.float32
BF16 = jnp.bfloat16
LAG = 12


def layer_kernel(
    sizes,
    q_ref,
    k_ref,
    v_ref,
    lg_ref,
    res_ref,
    ow_ref,
    mix_gain_ref,
    ffn_gain_ref,
    out_gain_ref,
    gate_ref,
    up_ref,
    down_ref,
    out_ref,
    kv_all,
    m_all,
    o_all,
    d_all,
    ow_all,
    att_all,
    mixed,
    middle,
    normed,
    m_act,
    o_act,
    hidden,
    parts,
    rs_buf,
    ffn,
    upper,
    acc_near,
    run_near,
    acc_far,
    local_sem,
    kv_send,
    kv_recv,
    m_send,
    m_recv,
    d_send,
    d_recv,
    y_send,
    y_recv,
    ow_send,
    ow_recv,
    ow_pass_send,
    ow_pass_recv,
    att_send,
    att_recv,
    rs_send,
    rs_recv,
    ag_send,
    ag_recv,
):
    n, t = sizes
    tok, width = q_ref.shape
    w_rows = gate_ref.shape[0]
    half_rows = w_rows // 2
    d_model = res_ref.shape[1]
    first_steps, second_steps = n // 2, n - 1 - n // 2
    lag = min(LAG, first_steps)
    tile = 128
    tile_pairs = d_model // tile // 2
    own_rows = tok // t
    grp, i, c = lax.axis_index("grp"), lax.axis_index("sp"), lax.axis_index("tp")
    parity = lax.rem(grp, 2)
    partner = grp + 1 - 2 * parity
    sibling = c + 1 - 2 * lax.rem(c, 2)
    right, left = lax.rem(i + 1, n), lax.rem(i + n - 1, n)

    def peer(k):
        return lax.rem(c + k, t)

    kv_own = kv_all.at[i]
    w_own = pl.ds(pl.multiple_of(i * w_rows, w_rows), w_rows)
    copies = [
        pltpu.make_async_copy(k_ref, kv_own.at[pl.ds(0, tok)], local_sem.at[0]),
        pltpu.make_async_copy(v_ref, kv_own.at[pl.ds(tok, tok)], local_sem.at[1]),
        pltpu.make_async_copy(lg_ref, kv_own.at[pl.ds(2 * tok, 16)], local_sem.at[2]),
        pltpu.make_async_copy(down_ref, d_all.at[w_own], local_sem.at[3]),
        pltpu.make_async_copy(
            ow_ref, ow_all.at[pl.ds(pl.multiple_of(c * width, width), width)], local_sem.at[4]
        ),
    ]
    for copy in copies:
        copy.start()

    @pl.when(parity == 0)
    def _():
        pltpu.make_async_copy(gate_ref, m_all.at[w_own], local_sem.at[5]).start()
        pltpu.make_async_copy(up_ref, o_all.at[w_own], local_sem.at[6]).start()

    @pl.when(parity == 1)
    def _():
        pltpu.make_async_copy(up_ref, m_all.at[w_own], local_sem.at[5]).start()
        pltpu.make_async_copy(gate_ref, o_all.at[w_own], local_sem.at[6]).start()

    barrier = pltpu.get_barrier_semaphore()
    for where in [{"sp": right}, {"sp": left}, {"grp": partner}] + [
        {"tp": peer(k)} for k in range(1, t)
    ]:
        pl.semaphore_signal(barrier, inc=1, device_id=where, device_id_type=MESH)

    rows = lax.broadcasted_iota(jnp.int32, (tile, 2 * tile), 0)
    cols = lax.broadcasted_iota(jnp.int32, (tile, 2 * tile), 1)
    upper[...] = jnp.where((rows > cols) | (cols >= tile), 1.0, 0.0).astype(BF16)
    acc_far[...] = jnp.zeros_like(acc_far)

    for copy in copies:
        copy.wait()
    pltpu.make_async_copy(gate_ref, m_all.at[w_own], local_sem.at[5]).wait()
    pltpu.make_async_copy(up_ref, o_all.at[w_own], local_sem.at[6]).wait()
    pl.semaphore_wait(barrier, t + 2)

    def block_at(direction, back):
        return lax.rem(i + n - back, n) if direction == 0 else lax.rem(i + back, n)

    def kv_copy(direction, step, back):
        block = kv_all.at[block_at(direction, back)]
        return pltpu.make_async_remote_copy(
            src_ref=block,
            dst_ref=block,
            send_sem=kv_send,
            recv_sem=kv_recv.at[direction, step - 1],
            device_id={"sp": right if direction == 0 else left},
            device_id_type=MESH,
        )

    def half_of(direction, back, half):
        start = block_at(direction, back) * w_rows + half * half_rows
        return pl.ds(pl.multiple_of(start, half_rows), half_rows)

    def w_copy(ref, send, recv, direction, step, back, half):
        part = ref.at[half_of(direction, back, half)]
        return pltpu.make_async_remote_copy(
            src_ref=part,
            dst_ref=part,
            send_sem=send,
            recv_sem=recv.at[direction, half, step - 1],
            device_id={"sp": right if direction == 0 else left},
            device_id_type=MESH,
        )

    def steps_of(direction, flipped):
        return first_steps if direction == int(flipped) else second_steps

    def if_step(condition, body):
        if isinstance(condition, bool):
            if condition:
                body()
        else:
            pl.when(condition)(body)

    def kv_slot(s):
        for direction in (0, 1):
            count = steps_of(direction, False)

            def arrived(direction=direction, count=count):
                kv_copy(direction, s, s).wait_recv()
                if_step(s < count, lambda: kv_copy(direction, s + 1, s).start())

            if_step(s <= count, arrived)

    def w_slot(ref, send, recv, s, flipped, to_partner):
        for half in (0, 1):
            for direction in (0, 1):
                count = steps_of(direction, flipped)

                def arrived(direction=direction, count=count, half=half):
                    w_copy(ref, send, recv, direction, s, s, half).wait_recv()
                    if_step(
                        s < count,
                        lambda: w_copy(ref, send, recv, direction, s + 1, s, half).start(),
                    )
                    if to_partner:
                        part = half_of(direction, s, half)
                        pltpu.make_async_remote_copy(
                            src_ref=m_all.at[part],
                            dst_ref=o_all.at[part],
                            send_sem=y_send,
                            recv_sem=y_recv,
                            device_id={"grp": partner},
                            device_id_type=MESH,
                        ).start()

                if_step(s <= count, arrived)

    def m_slot(s):
        w_slot(m_all, m_send, m_recv, s, True, True)

    def d_slot(s):
        w_slot(d_all, d_send, d_recv, s, False, False)

    def d_first():
        for half in (0, 1):
            for direction in (0, 1):
                w_copy(d_all, d_send, d_recv, direction, 1, 0, half).start()

    for direction in (0, 1):
        kv_copy(direction, 1, 0).start()
    for half in (0, 1):
        for direction in (0, 1):
            w_copy(m_all, m_send, m_recv, direction, 1, 0, half).start()

    def ow_block(index):
        return ow_all.at[pl.ds(pl.multiple_of(index * width, width), width)]

    def ow_copy(index, where, send, recv):
        return pltpu.make_async_remote_copy(
            src_ref=ow_block(index),
            dst_ref=ow_block(index),
            send_sem=send,
            recv_sem=recv,
            device_id={"tp": where},
            device_id_type=MESH,
        )

    for k in range(2, t, 2):
        ow_copy(c, peer(k), ow_send, ow_recv).start()
    ow_copy(c, sibling, ow_pass_send, ow_pass_recv).start()

    scale = width ** (-0.5)

    def terms(block, causal):
        k = kv_all[block, pl.ds(0, tok), :]
        v = kv_all[block, pl.ds(tok, tok), :]
        logit = kv_all[block, pl.ds(2 * tok, 16), :].astype(F32)[0:1, :]
        scores = lax.dot_general(
            q_ref[...], k, (((1,), (1,)), ((), ())), preferred_element_type=F32
        )
        scores = scores * scale + logit
        soft = jnp.log1p(jnp.exp(-jnp.abs(scores)))
        keep = -(jnp.maximum(scores, 0.0) + soft)
        if causal is not None:
            keep = jnp.where(causal, keep, 0.0)
        high = keep.astype(BF16)
        low = (keep - high.astype(F32)).astype(BF16)
        u = upper[...]
        sums = jnp.dot(high, u, preferred_element_type=F32) + jnp.dot(
            low, u, preferred_element_type=F32
        )
        within, total = sums[:, :tile], sums[:, tile:]
        stick = jnp.exp(jnp.minimum(scores, 0.0) - soft + within)
        if causal is not None:
            stick = jnp.where(causal, stick, 0.0)
        part = jnp.dot(stick.astype(BF16), v, preferred_element_type=F32)
        return total, part

    def attend(s):
        @pl.when(i >= s)
        def _():
            total, part = terms(i - s, None)
            so_far = run_near[...]
            acc_near[...] += jnp.exp(so_far) * part
            run_near[...] = so_far + total

        @pl.when((i + s >= n) & (s <= second_steps))
        def _():
            total, part = terms(i + s - n, None)
            acc_far[...] = acc_far[...] * jnp.exp(total) + part

    q_pos = lax.broadcasted_iota(jnp.int32, (tok, tok), 0)
    k_pos = lax.broadcasted_iota(jnp.int32, (tok, tok), 1)
    total, part = terms(i, k_pos < q_pos)
    acc_near[...] = part
    run_near[...] = total

    def early(s, carry):
        kv_slot(s)
        m_slot(s)
        attend(s)
        return carry

    def middle_slots(s, carry):
        kv_slot(s)
        m_slot(s)
        d_slot(s - lag)
        attend(s)
        return carry

    if lag > 0:
        lax.fori_loop(1, lag + 1, early, 0)
    d_first()
    if lag < first_steps:
        lax.fori_loop(lag + 1, first_steps + 1, middle_slots, 0)

    def columns(index, size):
        return pl.ds(pl.multiple_of(index * size, size), size)

    def send_attended():
        own = columns(c, width)
        att_all[:, own] = (acc_near[...] + jnp.exp(run_near[...]) * acc_far[...]).astype(BF16)
        if t > 2:
            x_rows = ow_all.at[pl.ds(0, (t // 2 - 1) * width)]
            pltpu.make_async_copy(x_rows, x_rows, ow_recv).wait()
            for k in range(2, t, 2):
                ow_copy(peer(k), sibling, ow_pass_send, ow_pass_recv).start()
        for k in range(1, t):
            pltpu.make_async_remote_copy(
                src_ref=att_all.at[:, own],
                dst_ref=att_all.at[:, own],
                send_sem=att_send,
                recv_sem=att_recv,
                device_id={"tp": peer(k)},
                device_id_type=MESH,
            ).start()

    wide = 256

    def wait_attended():
        others = att_all.at[:, pl.ds(0, (t - 1) * width)]
        pltpu.make_async_copy(others, others, att_recv).wait()
        passed = ow_all.at[pl.ds(0, (t // 2) * width)]
        pltpu.make_async_copy(passed, passed, ow_pass_recv).wait()

    def project():
        def step(j, carry):
            at = columns(j, wide)
            mixed[:, at] = jnp.dot(
                att_all[...], ow_all[:, at], preferred_element_type=F32
            ).astype(BF16)
            return carry

        lax.fori_loop(0, d_model // wide, step, 0)

    def normalize(x):
        return x * lax.rsqrt(jnp.mean(x * x, axis=-1, keepdims=True) + EPSILON)

    chunk = 16

    def norms():
        def step(j, carry):
            at = columns(j, chunk)
            mid = (
                res_ref[at, :].astype(F32)
                + mix_gain_ref[...] * normalize(mixed[at, :].astype(F32))
            ).astype(BF16)
            middle[at, :] = mid
            normed[at, :] = (ffn_gain_ref[...] * normalize(mid.astype(F32))).astype(BF16)
            return carry

        lax.fori_loop(0, tok // chunk, step, 0)

    def act_of(weights, act):
        act[...] = jnp.zeros_like(act)

        def step(j, carry):
            at = columns(j, wide)
            act[...] += jnp.dot(normed[:, at], weights[at, :], preferred_element_type=F32)
            return carry

        lax.fori_loop(0, d_model // wide, step, 0)

    def mine():
        act_of(m_all, m_act)

    def other():
        rest = o_all.at[pl.ds(0, (n - 1) * w_rows)]
        pltpu.make_async_copy(rest, rest, y_recv).wait()
        act_of(o_all, o_act)

    def hide():
        def step(j, carry):
            at = columns(j, chunk)
            a, b = m_act[at, :], o_act[at, :]
            gate = jnp.where(parity == 0, a, b)
            up = jnp.where(parity == 0, b, a)
            hidden[at, :] = (gate / (1.0 + jnp.exp(-gate)) * up).astype(BF16)
            return carry

        lax.fori_loop(0, tok // chunk, step, 0)

    count = d_model // tile
    own = pl.ds(pl.multiple_of(c * own_rows, own_rows), own_rows)

    def tiles_of(k):
        h, odd = i // 2, lax.rem(i, 2)
        return lax.rem(h - k + odd + count, count), lax.rem(h + k - 1 + odd, count)

    def partial_pair(k):
        for p in tiles_of(k):
            parts[p] = lax.dot_general(
                hidden[...],
                d_all[columns(p, tile), :],
                (((1,), (1,)), ((), ())),
                preferred_element_type=F32,
            ).astype(BF16)
            for far in range(1, t):
                rows_of = pl.ds(pl.multiple_of(peer(far) * own_rows, own_rows), own_rows)
                pltpu.make_async_remote_copy(
                    src_ref=parts.at[p, rows_of],
                    dst_ref=rs_buf.at[p, far - 1],
                    send_sem=rs_send,
                    recv_sem=rs_recv.at[p],
                    device_id={"tp": peer(far)},
                    device_id_type=MESH,
                ).start()

    def reduce_pair(k):
        for p in tiles_of(k):
            pltpu.make_async_copy(rs_buf.at[p], rs_buf.at[p], rs_recv.at[p]).wait()
            total = parts[p, own, :].astype(F32)
            for far in range(1, t):
                total = total + rs_buf[p, far - 1].astype(F32)
            ffn[p, own, :] = total.astype(BF16)
            for far in range(1, t):
                pltpu.make_async_remote_copy(
                    src_ref=ffn.at[p, own],
                    dst_ref=ffn.at[p, own],
                    send_sem=ag_send,
                    recv_sem=ag_recv.at[p],
                    device_id={"tp": peer(far)},
                    device_id_type=MESH,
                ).start()

    tasks = [
        send_attended,
        lambda: (wait_attended(), project()),
        norms,
        mine,
        other,
        hide,
    ]
    done_parts, done_sums = 0, 0

    def advance(ready, most):
        nonlocal done_parts, done_sums
        sums = done_parts
        for _ in range(most):
            if done_parts < ready:
                done_parts += 1
                partial_pair(done_parts)
        while done_sums < sums:
            done_sums += 1
            reduce_pair(done_sums)

    for s in range(first_steps - lag + 1, first_steps + 1):
        d_slot(s)
        if tasks:
            tasks.pop(0)()
        else:
            advance(s // 2, 2)
    while tasks:
        tasks.pop(0)()
    while done_sums < tile_pairs:
        advance(tile_pairs, tile_pairs)

    for p in range(count):
        others = rs_buf.at[p]
        pltpu.make_async_copy(others, others, ag_recv.at[p]).wait()

    def finish(j, carry):
        at = columns(j, chunk)
        x = jnp.concatenate([ffn[p, at, :] for p in range(count)], axis=1).astype(F32)
        out_ref[at, :] = (
            middle[at, :].astype(F32) + out_gain_ref[...] * normalize(x)
        ).astype(BF16)
        return carry

    lax.fori_loop(0, tok // chunk, finish, 0)

    def drain(ref, sem):
        pltpu.make_async_copy(ref, ref, sem).wait()

    drain(kv_all.at[pl.ds(0, n - 1)], kv_send)
    ring = pl.ds(0, (n - 1) * w_rows)
    drain(m_all.at[ring], m_send)
    drain(m_all.at[ring], y_send)
    drain(d_all.at[ring], d_send)
    if t > 2:
        drain(ow_all.at[pl.ds(0, (t // 2 - 1) * width)], ow_send)
    drain(ow_all.at[pl.ds(0, (t // 2) * width)], ow_pass_send)
    drain(att_all.at[:, pl.ds(0, (t - 1) * width)], att_send)
    drain(rs_buf, rs_send)
    drain(rs_buf, ag_send)


def solution(mesh):
    n, t = mesh.shape["sp"], mesh.shape["tp"]

    def shards(
        query_rows,
        key_rows,
        value_rows,
        key_logit,
        residual,
        out_weight,
        mix_gain,
        ffn_gain,
        out_gain,
        gate_weight,
        up_weight,
        down_weight,
    ):
        tok, width = query_rows.shape
        w_rows, units = gate_weight.shape
        d_model = residual.shape[1]
        tile = 128
        count = d_model // tile
        logit = jnp.broadcast_to(key_logit.reshape(1, tok), (16, tok))
        vmem = pl.BlockSpec(memory_space=pltpu.VMEM)
        anywhere = pl.BlockSpec(memory_space=pl.ANY)
        steps = n // 2
        dma = pltpu.SemaphoreType.DMA
        return pl.pallas_call(
            functools.partial(layer_kernel, (n, t)),
            out_shape=jax.ShapeDtypeStruct((tok, d_model), BF16),
            in_specs=[vmem] + [anywhere] * 3 + [vmem, anywhere] + [vmem] * 3 + [anywhere] * 3,
            out_specs=vmem,
            scratch_shapes=[
                pltpu.VMEM((n, 2 * tok + 16, width), BF16),
                pltpu.VMEM((n * w_rows, units), BF16),
                pltpu.VMEM((n * w_rows, units), BF16),
                pltpu.VMEM((n * w_rows, units), BF16),
                pltpu.VMEM((t * width, d_model), BF16),
                pltpu.VMEM((tok, t * width), BF16),
                pltpu.VMEM((tok, d_model), BF16),
                pltpu.VMEM((tok, d_model), BF16),
                pltpu.VMEM((tok, d_model), BF16),
                pltpu.VMEM((tok, units), F32),
                pltpu.VMEM((tok, units), F32),
                pltpu.VMEM((tok, units), BF16),
                pltpu.VMEM((count, tok, tile), BF16),
                pltpu.VMEM((count, t - 1, tok // t, tile), BF16),
                pltpu.VMEM((count, tok, tile), BF16),
                pltpu.VMEM((tile, 2 * tile), BF16),
                pltpu.VMEM((tok, width), F32),
                pltpu.VMEM((tok, width), F32),
                pltpu.VMEM((tok, width), F32),
                dma((7,)),
                dma,
                dma((2, steps)),
                dma,
                dma((2, 2, steps)),
                dma,
                dma((2, 2, steps)),
                dma,
                dma,
                dma,
                dma,
                dma,
                dma,
                dma,
                dma,
                dma,
                dma((count,)),
                dma,
                dma((count,)),
            ],
            compiler_params=pltpu.CompilerParams(
                collective_id=0, has_side_effects=True, vmem_limit_bytes=48 * 1024 * 1024
            ),
            name="layer",
        )(
            query_rows,
            key_rows,
            value_rows,
            logit,
            residual,
            out_weight,
            mix_gain.reshape(1, d_model),
            ffn_gain.reshape(1, d_model),
            out_gain.reshape(1, d_model),
            gate_weight,
            up_weight,
            down_weight,
        )

    rows = P(("grp", "sp"), "tp")
    placed = (
        rows,
        rows,
        rows,
        rows,
        P(("grp", "sp"), None),
        P("tp", None),
        P(),
        P(),
        P(),
        P("sp", "tp"),
        P("sp", "tp"),
        P("sp", "tp"),
    )
    return jax.shard_map(
        shards, mesh=mesh, in_specs=placed, out_specs=P(("grp", "sp"), None), check_vma=False
    )
```

```python
import functools

import jax
import jax.numpy as jnp
from jax import lax
from jax.experimental import pallas as pl
from jax.experimental.pallas import tpu as pltpu
from jax.sharding import PartitionSpec as P

EPSILON = 1e-06
MESH = pl.DeviceIdType.MESH
F32 = jnp.float32
BF16 = jnp.bfloat16
WIDE = 256


def layer_kernel(
    sizes,
    q_in,
    k_ref,
    v_ref,
    lg_ref,
    res_in,
    ow_ref,
    mix_gain_in,
    ffn_gain_in,
    out_gain_in,
    gate_ref,
    up_ref,
    down_ref,
    out_ref,
    q_ref,
    res_ref,
    mix_gain_ref,
    ffn_gain_ref,
    out_gain_ref,
    kv_all,
    m_all,
    o_all,
    d_all,
    ow_all,
    att_all,
    mixed,
    middle,
    normed,
    m_act,
    o_act,
    hidden,
    parts,
    rs_buf,
    ffn,
    upper,
    acc_near,
    run_near,
    acc_far,
    local_sem,
    kv_send,
    kv_recv,
    m_send,
    m_recv,
    d_send,
    d_recv,
    y_send,
    y_recv,
    ow_send,
    ow_recv,
    ow_pass_send,
    ow_pass_recv,
    att_send,
    att_recv,
    rs_send,
    rs_recv,
    ag_send,
    ag_recv,
):
    n, t = sizes
    tok, width = q_in.shape
    w_rows = gate_ref.shape[0]
    half_rows = w_rows // 2
    d_model = res_ref.shape[1]
    first_steps, second_steps = n // 2, n - 1 - n // 2
    tile, wide = 128, WIDE
    own_rows = tok // t
    grp, i, c = lax.axis_index("grp"), lax.axis_index("sp"), lax.axis_index("tp")
    parity = lax.rem(grp, 2)
    partner = grp + 1 - 2 * parity
    sibling = c + 1 - 2 * lax.rem(c, 2)
    right, left = lax.rem(i + 1, n), lax.rem(i + n - 1, n)

    def peer(k):
        return lax.rem(c + k, t)

    kv_own = kv_all.at[i]
    w_own = pl.ds(pl.multiple_of(i * w_rows, w_rows), w_rows)
    copies = [
        pltpu.make_async_copy(k_ref, kv_own.at[pl.ds(0, tok)], local_sem.at[0]),
        pltpu.make_async_copy(v_ref, kv_own.at[pl.ds(tok, tok)], local_sem.at[1]),
        pltpu.make_async_copy(lg_ref, kv_own.at[pl.ds(2 * tok, 16)], local_sem.at[2]),
        pltpu.make_async_copy(down_ref, d_all.at[w_own], local_sem.at[3]),
        pltpu.make_async_copy(
            ow_ref, ow_all.at[pl.ds(pl.multiple_of(c * width, width), width)], local_sem.at[4]
        ),
        pltpu.make_async_copy(q_in, q_ref, local_sem.at[7]),
        pltpu.make_async_copy(res_in, res_ref, local_sem.at[8]),
        pltpu.make_async_copy(mix_gain_in, mix_gain_ref, local_sem.at[9]),
        pltpu.make_async_copy(ffn_gain_in, ffn_gain_ref, local_sem.at[10]),
        pltpu.make_async_copy(out_gain_in, out_gain_ref, local_sem.at[11]),
    ]
    for copy in copies:
        copy.start()

    @pl.when(parity == 0)
    def _():
        pltpu.make_async_copy(gate_ref, m_all.at[w_own], local_sem.at[5]).start()
        pltpu.make_async_copy(up_ref, o_all.at[w_own], local_sem.at[6]).start()

    @pl.when(parity == 1)
    def _():
        pltpu.make_async_copy(up_ref, m_all.at[w_own], local_sem.at[5]).start()
        pltpu.make_async_copy(gate_ref, o_all.at[w_own], local_sem.at[6]).start()

    barrier = pltpu.get_barrier_semaphore()
    for where in [{"sp": right}, {"sp": left}, {"grp": partner}] + [
        {"tp": peer(k)} for k in range(1, t)
    ]:
        pl.semaphore_signal(barrier, inc=1, device_id=where, device_id_type=MESH)

    rows = lax.broadcasted_iota(jnp.int32, (tile, 2 * tile), 0)
    cols = lax.broadcasted_iota(jnp.int32, (tile, 2 * tile), 1)
    upper[...] = jnp.where((rows > cols) | (cols >= tile), 1.0, 0.0).astype(BF16)
    acc_far[...] = jnp.zeros_like(acc_far)

    with jax.named_scope("local"):
        for copy in copies:
            copy.wait()
        pltpu.make_async_copy(gate_ref, m_all.at[w_own], local_sem.at[5]).wait()
        pltpu.make_async_copy(up_ref, o_all.at[w_own], local_sem.at[6]).wait()
    with jax.named_scope("barrier"):
        pl.semaphore_wait(barrier, t + 2)

    def block_at(direction, back):
        return lax.rem(i + n - back, n) if direction == 0 else lax.rem(i + back, n)

    def kv_copy(direction, step, back):
        block = kv_all.at[block_at(direction, back)]
        return pltpu.make_async_remote_copy(
            src_ref=block,
            dst_ref=block,
            send_sem=kv_send,
            recv_sem=kv_recv.at[direction, step - 1],
            device_id={"sp": right if direction == 0 else left},
            device_id_type=MESH,
        )

    def half_of(direction, back, half):
        start = block_at(direction, back) * w_rows + half * half_rows
        return pl.ds(pl.multiple_of(start, half_rows), half_rows)

    def w_copy(ref, send, recv, direction, step, back, half):
        part = ref.at[half_of(direction, back, half)]
        return pltpu.make_async_remote_copy(
            src_ref=part,
            dst_ref=part,
            send_sem=send,
            recv_sem=recv.at[direction, half, step - 1],
            device_id={"sp": right if direction == 0 else left},
            device_id_type=MESH,
        )

    def steps_of(direction, flipped):
        return first_steps if direction == int(flipped) else second_steps

    def if_step(condition, body):
        if isinstance(condition, bool):
            if condition:
                body()
        else:
            pl.when(condition)(body)

    def kv_slot(s):
        for direction in (0, 1):
            count = steps_of(direction, False)

            def arrived(direction=direction, count=count):
                kv_copy(direction, s, s).wait_recv()
                if_step(s < count, lambda: kv_copy(direction, s + 1, s).start())

            if_step(s <= count, arrived)

    def w_arrived(ref, send, recv, s, half, direction, count):
        w_copy(ref, send, recv, direction, s, s, half).wait_recv()
        if_step(s < count, lambda: w_copy(ref, send, recv, direction, s + 1, s, half).start())

    def to_partner(s, half, direction):
        part = m_all.at[half_of(direction, s, half)]
        pltpu.make_async_remote_copy(
            src_ref=part,
            dst_ref=o_all.at[half_of(direction, s, half)],
            send_sem=y_send,
            recv_sem=y_recv.at[s - 1],
            device_id={"grp": partner},
            device_id_type=MESH,
        ).start()

    def w_slot(s, half):
        for direction in (0, 1):

            def m_arrived(direction=direction, count=steps_of(direction, True)):
                w_arrived(m_all, m_send, m_recv, s, half, direction, count)
                to_partner(s, half, direction)

            if_step(s <= steps_of(direction, True), m_arrived)
        for direction in (0, 1):

            def d_arrived(direction=direction, count=steps_of(direction, False)):
                w_arrived(d_all, d_send, d_recv, s, half, direction, count)

            if_step(s <= steps_of(direction, False), d_arrived)

    for direction in (0, 1):
        kv_copy(direction, 1, 0).start()
    for half in (0, 1):
        for direction in (0, 1):
            w_copy(m_all, m_send, m_recv, direction, 1, 0, half).start()
        for direction in (0, 1):
            w_copy(d_all, d_send, d_recv, direction, 1, 0, half).start()

    def ow_block(index):
        return ow_all.at[pl.ds(pl.multiple_of(index * width, width), width)]

    def ow_copy(index, where, send, recv):
        return pltpu.make_async_remote_copy(
            src_ref=ow_block(index),
            dst_ref=ow_block(index),
            send_sem=send,
            recv_sem=recv,
            device_id={"tp": where},
            device_id_type=MESH,
        )

    for k in range(2, t, 2):
        ow_copy(c, peer(k), ow_send, ow_recv).start()
    ow_copy(c, sibling, ow_pass_send, ow_pass_recv).start()

    scale = width ** (-0.5)

    def terms(block, causal):
        k = kv_all[block, pl.ds(0, tok), :]
        v = kv_all[block, pl.ds(tok, tok), :]
        logit = kv_all[block, pl.ds(2 * tok, 16), :].astype(F32)[0:1, :]
        scores = lax.dot_general(
            q_ref[...], k, (((1,), (1,)), ((), ())), preferred_element_type=F32
        )
        scores = scores * scale + logit
        soft = jnp.log1p(jnp.exp(-jnp.abs(scores)))
        keep = -(jnp.maximum(scores, 0.0) + soft)
        if causal is not None:
            keep = jnp.where(causal, keep, 0.0)
        high = keep.astype(BF16)
        low = (keep - high.astype(F32)).astype(BF16)
        u = upper[...]
        sums = jnp.dot(high, u, preferred_element_type=F32) + jnp.dot(
            low, u, preferred_element_type=F32
        )
        within, total = sums[:, :tile], sums[:, tile:]
        stick = jnp.exp(jnp.minimum(scores, 0.0) - soft + within)
        if causal is not None:
            stick = jnp.where(causal, stick, 0.0)
        part = jnp.dot(stick.astype(BF16), v, preferred_element_type=F32)
        return total, part

    def attend_near(s):
        @pl.when(i >= s)
        def _():
            total, part = terms(i - s, None)
            so_far = run_near[...]
            acc_near[...] += jnp.exp(so_far) * part
            run_near[...] = so_far + total

    def attend_far(s):
        @pl.when((i + s >= n) & (s <= second_steps))
        def _():
            total, part = terms(i + s - n, None)
            acc_far[...] = acc_far[...] * jnp.exp(total) + part

    q_pos = lax.broadcasted_iota(jnp.int32, (tok, tok), 0)
    k_pos = lax.broadcasted_iota(jnp.int32, (tok, tok), 1)
    total, part = terms(i, k_pos < q_pos)
    acc_near[...] = part
    run_near[...] = total

    def group(g, carry):
        s, w = 4 * g, 3 * g
        with jax.named_scope("kv1"):
            kv_slot(s + 1)
        attend_near(s + 1)
        with jax.named_scope("w1a"):
            w_slot(w + 1, 0)
        attend_far(s + 1)
        with jax.named_scope("w1b"):
            w_slot(w + 1, 1)
        with jax.named_scope("kv2"):
            kv_slot(s + 2)
        attend_near(s + 2)
        with jax.named_scope("w2a"):
            w_slot(w + 2, 0)
        attend_far(s + 2)
        with jax.named_scope("kv3"):
            kv_slot(s + 3)
        attend_near(s + 3)
        with jax.named_scope("w2b"):
            w_slot(w + 2, 1)
        attend_far(s + 3)
        with jax.named_scope("w3a"):
            w_slot(w + 3, 0)
        with jax.named_scope("kv4"):
            kv_slot(s + 4)
        attend_near(s + 4)
        with jax.named_scope("w3b"):
            w_slot(w + 3, 1)
        attend_far(s + 4)
        return carry

    groups = first_steps // 4
    early = 3 * groups
    lax.fori_loop(0, groups, group, 0)

    def columns(index, size):
        return pl.ds(pl.multiple_of(index * size, size), size)

    def send_attended():
        own = columns(c, width)
        att_all[:, own] = (acc_near[...] + jnp.exp(run_near[...]) * acc_far[...]).astype(BF16)
        if t > 2:
            x_rows = ow_all.at[pl.ds(0, (t // 2 - 1) * width)]
            pltpu.make_async_copy(x_rows, x_rows, ow_recv).wait()
            for k in range(2, t, 2):
                ow_copy(peer(k), sibling, ow_pass_send, ow_pass_recv).start()
        for k in range(1, t):
            pltpu.make_async_remote_copy(
                src_ref=att_all.at[:, own],
                dst_ref=att_all.at[:, own],
                send_sem=att_send,
                recv_sem=att_recv,
                device_id={"tp": peer(k)},
                device_id_type=MESH,
            ).start()


    def wait_attended():
        others = att_all.at[:, pl.ds(0, (t - 1) * width)]
        pltpu.make_async_copy(others, others, att_recv).wait()
        passed = ow_all.at[pl.ds(0, (t // 2) * width)]
        pltpu.make_async_copy(passed, passed, ow_pass_recv).wait()

    def project(start, stop):
        def step(j, carry):
            at = columns(j, wide)
            mixed[:, at] = jnp.dot(
                att_all[...], ow_all[:, at], preferred_element_type=F32
            ).astype(BF16)
            return carry

        lax.fori_loop(start, stop, step, 0)

    def normalize(x):
        return x * lax.rsqrt(jnp.mean(x * x, axis=-1, keepdims=True) + EPSILON)

    chunk = 16

    def norms(start, stop):
        def step(j, carry):
            at = columns(j, chunk)
            mid = (
                res_ref[at, :].astype(F32)
                + mix_gain_ref[...] * normalize(mixed[at, :].astype(F32))
            ).astype(BF16)
            middle[at, :] = mid
            normed[at, :] = (ffn_gain_ref[...] * normalize(mid.astype(F32))).astype(BF16)
            return carry

        lax.fori_loop(start, stop, step, 0)

    chunks, per_chunk = d_model // wide, wide // w_rows
    arrived_chunks = max(0, min(chunks, (2 * early + 2 - per_chunk) // per_chunk))
    first_chunk = (i + n - early + per_chunk - 1) // per_chunk

    def act_of(weights, act, start, stop):
        def step(j, carry):
            at = columns(lax.rem(first_chunk + j, chunks), wide)
            act[...] += jnp.dot(normed[:, at], weights[at, :], preferred_element_type=F32)
            return carry

        lax.fori_loop(start, stop, step, 0)

    def wait_other(start, stop):
        for s in range(start, stop):
            blocks = int(s <= first_steps) + int(s <= second_steps)
            rest = o_all.at[pl.ds(0, blocks * w_rows)]
            pltpu.make_async_copy(rest, rest, y_recv.at[s - 1]).wait()

    def hide():
        def step(j, carry):
            at = columns(j, chunk)
            a, b = m_act[at, :], o_act[at, :]
            gate = jnp.where(parity == 0, a, b)
            up = jnp.where(parity == 0, b, a)
            hidden[at, :] = (gate / (1.0 + jnp.exp(-gate)) * up).astype(BF16)
            return carry

        lax.fori_loop(0, tok // chunk, step, 0)

    count = d_model // wide
    own = pl.ds(pl.multiple_of(c * own_rows, own_rows), own_rows)

    def partial(p, carry):
        parts[p] = lax.dot_general(
            hidden[...],
            d_all[columns(p, wide), :],
            (((1,), (1,)), ((), ())),
            preferred_element_type=F32,
        ).astype(BF16)
        for far in range(1, t):
            rows_of = pl.ds(pl.multiple_of(peer(far) * own_rows, own_rows), own_rows)
            pltpu.make_async_remote_copy(
                src_ref=parts.at[p, rows_of],
                dst_ref=rs_buf.at[p, far - 1],
                send_sem=rs_send,
                recv_sem=rs_recv.at[p],
                device_id={"tp": peer(far)},
                device_id_type=MESH,
            ).start()
        return carry

    def total_of(p, carry):
        pltpu.make_async_copy(rs_buf.at[p], rs_buf.at[p], rs_recv.at[p]).wait()
        total = parts[p, own, :].astype(F32)
        for far in range(1, t):
            total = total + rs_buf[p, far - 1].astype(F32)
        ffn[p, own, :] = total.astype(BF16)
        for far in range(1, t):
            pltpu.make_async_remote_copy(
                src_ref=ffn.at[p, own],
                dst_ref=ffn.at[p, own],
                send_sem=ag_send,
                recv_sem=ag_recv.at[p],
                device_id={"tp": peer(far)},
                device_id_type=MESH,
            ).start()
        return carry

    def zero_acts():
        m_act[...] = jnp.zeros_like(m_act)
        o_act[...] = jnp.zeros_like(o_act)

    n_cols, n_rows = d_model // wide, tok // chunk
    some = arrived_chunks // 2

    def named(name, *bodies):
        def run():
            with jax.named_scope(name):
                for body in bodies:
                    body()

        return run

    tasks = [
        named("zero", zero_acts),
        named("project1", wait_attended, lambda: project(0, n_cols // 2)),
        named("project2", lambda: project(n_cols // 2, n_cols)),
        named("norms1", lambda: norms(0, n_rows // 2)),
        named("norms2", lambda: norms(n_rows // 2, n_rows)),
        named("mine1", lambda: act_of(m_all, m_act, 0, some)),
        named("mine2", lambda: act_of(m_all, m_act, some, arrived_chunks)),
        named(
            "other1",
            lambda: wait_other(1, early + 1),
            lambda: act_of(o_all, o_act, 0, arrived_chunks),
        ),
    ]
    with jax.named_scope("send_attended"):
        send_attended()
    for s in range(early + 1, first_steps + 1):
        for half in (0, 1):
            with jax.named_scope("wl"):
                w_slot(s, half)
            if tasks:
                tasks.pop(0)()
    while tasks:
        tasks.pop(0)()
    with jax.named_scope("mine3"):
        act_of(m_all, m_act, arrived_chunks, chunks)
    with jax.named_scope("other2"):
        wait_other(early + 1, first_steps + 1)
        act_of(o_all, o_act, arrived_chunks, chunks)
    with jax.named_scope("hide"):
        hide()
    with jax.named_scope("partial"):
        lax.fori_loop(0, count, partial, 0)
    with jax.named_scope("total"):
        lax.fori_loop(0, count, total_of, 0)

    with jax.named_scope("gathered"):
        for p in range(count):
            others = rs_buf.at[p]
            pltpu.make_async_copy(others, others, ag_recv.at[p]).wait()

    def finish(j, carry):
        at = columns(j, chunk)
        x = jnp.concatenate([ffn[p, at, :] for p in range(count)], axis=1).astype(F32)
        out_ref[at, :] = (
            middle[at, :].astype(F32) + out_gain_ref[...] * normalize(x)
        ).astype(BF16)
        return carry

    with jax.named_scope("finish"):
        lax.fori_loop(0, tok // chunk, finish, 0)

    def drain(ref, sem):
        pltpu.make_async_copy(ref, ref, sem).wait()

    drain(kv_all.at[pl.ds(0, n - 1)], kv_send)
    ring = pl.ds(0, (n - 1) * w_rows)
    drain(m_all.at[ring], m_send)
    drain(m_all.at[ring], y_send)
    drain(d_all.at[ring], d_send)
    if t > 2:
        drain(ow_all.at[pl.ds(0, (t // 2 - 1) * width)], ow_send)
    drain(ow_all.at[pl.ds(0, (t // 2) * width)], ow_pass_send)
    drain(att_all.at[:, pl.ds(0, (t - 1) * width)], att_send)
    drain(rs_buf, rs_send)
    drain(rs_buf, ag_send)


def solution(mesh):
    n, t = mesh.shape["sp"], mesh.shape["tp"]

    def shards(
        query_rows,
        key_rows,
        value_rows,
        key_logit,
        residual,
        out_weight,
        mix_gain,
        ffn_gain,
        out_gain,
        gate_weight,
        up_weight,
        down_weight,
    ):
        tok, width = query_rows.shape
        w_rows, units = gate_weight.shape
        d_model = residual.shape[1]
        tile = 128
        count = d_model // WIDE
        logit = jnp.broadcast_to(key_logit.reshape(1, tok), (16, tok))
        vmem = pl.BlockSpec(memory_space=pltpu.VMEM)
        hbm = pl.BlockSpec(memory_space=pltpu.HBM)
        steps = n // 2
        dma = pltpu.SemaphoreType.DMA
        return pl.pallas_call(
            functools.partial(layer_kernel, (n, t)),
            out_shape=jax.ShapeDtypeStruct((tok, d_model), BF16),
            in_specs=[hbm] * 12,
            out_specs=vmem,
            scratch_shapes=[
                pltpu.VMEM((tok, width), BF16),
                pltpu.VMEM((tok, d_model), BF16),
                pltpu.VMEM((1, d_model), F32),
                pltpu.VMEM((1, d_model), F32),
                pltpu.VMEM((1, d_model), F32),
                pltpu.VMEM((n, 2 * tok + 16, width), BF16),
                pltpu.VMEM((n * w_rows, units), BF16),
                pltpu.VMEM((n * w_rows, units), BF16),
                pltpu.VMEM((n * w_rows, units), BF16),
                pltpu.VMEM((t * width, d_model), BF16),
                pltpu.VMEM((tok, t * width), BF16),
                pltpu.VMEM((tok, d_model), BF16),
                pltpu.VMEM((tok, d_model), BF16),
                pltpu.VMEM((tok, d_model), BF16),
                pltpu.VMEM((tok, units), F32),
                pltpu.VMEM((tok, units), F32),
                pltpu.VMEM((tok, units), BF16),
                pltpu.VMEM((count, tok, WIDE), BF16),
                pltpu.VMEM((count, t - 1, tok // t, WIDE), BF16),
                pltpu.VMEM((count, tok, WIDE), BF16),
                pltpu.VMEM((tile, 2 * tile), BF16),
                pltpu.VMEM((tok, width), F32),
                pltpu.VMEM((tok, width), F32),
                pltpu.VMEM((tok, width), F32),
                dma((12,)),
                dma,
                dma((2, steps)),
                dma,
                dma((2, 2, steps)),
                dma,
                dma((2, 2, steps)),
                dma,
                dma((steps,)),
                dma,
                dma,
                dma,
                dma,
                dma,
                dma,
                dma,
                dma((count,)),
                dma,
                dma((count,)),
            ],
            compiler_params=pltpu.CompilerParams(
                collective_id=0, has_side_effects=True, vmem_limit_bytes=67043328
            ),
            name="layer",
        )(
            query_rows,
            key_rows,
            value_rows,
            logit,
            residual,
            out_weight,
            mix_gain.reshape(1, d_model),
            ffn_gain.reshape(1, d_model),
            out_gain.reshape(1, d_model),
            gate_weight,
            up_weight,
            down_weight,
        )

    rows = P(("grp", "sp"), "tp")
    placed = (
        rows,
        rows,
        rows,
        rows,
        P(("grp", "sp"), None),
        P("tp", None),
        P(),
        P(),
        P(),
        P("sp", "tp"),
        P("sp", "tp"),
        P("sp", "tp"),
    )
    return jax.shard_map(
        shards, mesh=mesh, in_specs=placed, out_specs=P(("grp", "sp"), None), check_vma=False
    )
```

```python
import functools

import jax
import jax.numpy as jnp
from jax import lax
from jax.experimental import pallas as pl
from jax.experimental.pallas import tpu as pltpu
from jax.sharding import PartitionSpec as P

EPSILON = 1e-06
MESH = pl.DeviceIdType.MESH
F32 = jnp.float32
BF16 = jnp.bfloat16
WIDE = 256
LAST = 2
BEHIND = 3


def layer_kernel(
    sizes,
    q_in,
    k_ref,
    v_ref,
    lg_ref,
    res_in,
    ow_ref,
    mix_gain_in,
    ffn_gain_in,
    out_gain_in,
    gate_ref,
    up_ref,
    down_ref,
    out_ref,
    q_ref,
    res_ref,
    mix_gain_ref,
    ffn_gain_ref,
    out_gain_ref,
    kv_all,
    m_all,
    o_all,
    d_all,
    ow_all,
    att_all,
    mixed,
    middle,
    normed,
    m_act,
    o_act,
    hidden,
    parts,
    core_buf,
    halves,
    rs_buf,
    ffn,
    upper,
    acc_near,
    run_near,
    acc_far,
    local_sem,
    kv_send,
    kv_recv,
    m_send,
    m_recv,
    d_send,
    d_recv,
    y_send,
    y_recv,
    ow_send,
    ow_recv,
    ow_pass_send,
    ow_pass_recv,
    att_send,
    att_recv,
    rs_send,
    rs_recv,
    ag_send,
    ag_recv,
    cs_send,
    cs_recv,
    cg_send,
    cg_recv,
    dy_send,
    dy_recv,
    out,
    out_sem,
    rs_last,
    ls_send,
    ls_recv,
    lg_send,
    lg_recv,
):
    n, t = sizes
    tok, width = q_in.shape
    w_rows = gate_ref.shape[0]
    half_rows = w_rows // 2
    d_model = res_ref.shape[1]
    first_steps, second_steps = n // 2, n - 1 - n // 2
    tile, wide = 128, WIDE
    own_rows = tok // t
    grp, i, c = lax.axis_index("grp"), lax.axis_index("sp"), lax.axis_index("tp")
    parity = lax.rem(grp, 2)
    partner = grp + 1 - 2 * parity
    sibling = c + 1 - 2 * lax.rem(c, 2)
    right, left = lax.rem(i + 1, n), lax.rem(i + n - 1, n)

    def peer(k):
        return lax.rem(c + k, t)

    kv_own = kv_all.at[i]
    w_own = pl.ds(pl.multiple_of(i * w_rows, w_rows), w_rows)
    copies = [
        pltpu.make_async_copy(k_ref, kv_own.at[pl.ds(0, tok)], local_sem.at[0]),
        pltpu.make_async_copy(v_ref, kv_own.at[pl.ds(tok, tok)], local_sem.at[1]),
        pltpu.make_async_copy(lg_ref, kv_own.at[pl.ds(2 * tok, 16)], local_sem.at[2]),
        pltpu.make_async_copy(down_ref, d_all.at[w_own], local_sem.at[3]),
        pltpu.make_async_copy(
            ow_ref, ow_all.at[pl.ds(pl.multiple_of(c * width, width), width)], local_sem.at[4]
        ),
        pltpu.make_async_copy(q_in, q_ref, local_sem.at[7]),
        pltpu.make_async_copy(res_in, res_ref, local_sem.at[8]),
        pltpu.make_async_copy(mix_gain_in, mix_gain_ref, local_sem.at[9]),
        pltpu.make_async_copy(ffn_gain_in, ffn_gain_ref, local_sem.at[10]),
        pltpu.make_async_copy(out_gain_in, out_gain_ref, local_sem.at[11]),
    ]
    for copy in copies:
        copy.start()

    @pl.when(parity == 0)
    def _():
        pltpu.make_async_copy(gate_ref, m_all.at[w_own], local_sem.at[5]).start()
        pltpu.make_async_copy(up_ref, o_all.at[w_own], local_sem.at[6]).start()

    @pl.when(parity == 1)
    def _():
        pltpu.make_async_copy(up_ref, m_all.at[w_own], local_sem.at[5]).start()
        pltpu.make_async_copy(gate_ref, o_all.at[w_own], local_sem.at[6]).start()

    barrier = pltpu.get_barrier_semaphore()
    for where in [{"sp": right}, {"sp": left}, {"grp": partner}] + [
        {"tp": peer(k)} for k in range(1, t)
    ]:
        pl.semaphore_signal(barrier, inc=1, device_id=where, device_id_type=MESH)

    rows = lax.broadcasted_iota(jnp.int32, (tile, 2 * tile), 0)
    cols = lax.broadcasted_iota(jnp.int32, (tile, 2 * tile), 1)
    upper[...] = jnp.where((rows > cols) | (cols >= tile), 1.0, 0.0).astype(BF16)
    acc_far[...] = jnp.zeros_like(acc_far)

    with jax.named_scope("local"):
        for copy in copies:
            copy.wait()
        pltpu.make_async_copy(gate_ref, m_all.at[w_own], local_sem.at[5]).wait()
        pltpu.make_async_copy(up_ref, o_all.at[w_own], local_sem.at[6]).wait()
    with jax.named_scope("barrier"):
        pl.semaphore_wait(barrier, t + 2)

    def block_at(direction, back):
        return lax.rem(i + n - back, n) if direction == 0 else lax.rem(i + back, n)

    def kv_copy(direction, step, back, part):
        rows_of = pl.ds(0, tok) if part == 0 else pl.ds(tok, tok + 16)
        block = kv_all.at[block_at(direction, back), rows_of]
        return pltpu.make_async_remote_copy(
            src_ref=block,
            dst_ref=block,
            send_sem=kv_send.at[direction, part, step - 1],
            recv_sem=kv_recv.at[direction, part, step - 1],
            device_id={"sp": right if direction == 0 else left},
            device_id_type=MESH,
        )

    def half_of(direction, back, half):
        start = block_at(direction, back) * w_rows + half * half_rows
        return pl.ds(pl.multiple_of(start, half_rows), half_rows)

    quarter = half_rows // 2
    groups = first_steps // 4
    early = 3 * groups
    shared = max(0, early - BEHIND)

    def d_part(direction, back, part):
        if part == 0:
            return half_of(direction, back, 0)
        which = parity if part == 1 else 1 - parity
        start = block_at(direction, back) * w_rows + half_rows + which * quarter
        return pl.ds(pl.multiple_of(start, quarter), quarter)

    def w_copy(ref, send, recv, direction, step, half, rows_of):
        part = ref.at[rows_of]
        return pltpu.make_async_remote_copy(
            src_ref=part,
            dst_ref=part,
            send_sem=send,
            recv_sem=recv.at[direction, half, step - 1],
            device_id={"sp": right if direction == 0 else left},
            device_id_type=MESH,
        )

    def m_copy(direction, step, back, half):
        return w_copy(m_all, m_send, m_recv, direction, step, half, half_of(direction, back, half))

    def d_copy(direction, step, back, half):
        return w_copy(d_all, d_send, d_recv, direction, step, half, d_part(direction, back, half))

    def steps_of(direction, flipped):
        return first_steps if direction == int(flipped) else second_steps

    def if_step(condition, body):
        if isinstance(condition, bool):
            if condition:
                body()
        else:
            pl.when(condition)(body)

    def both(a, b):
        return (a and b) if isinstance(a, bool) else a & b

    def kv_moves(direction, step, back):
        if direction == 0:
            return (i >= back) & (i < n - 1) & (step <= first_steps)
        return (lax.rem(i + back, n) < second_steps) & (step <= second_steps)

    def kv_slot(s):
        for part in (0, 1):

            @pl.when((i >= s) & (s <= first_steps))
            def _(part=part):
                kv_copy(0, s, s, part).wait_recv()

            @pl.when(kv_moves(0, s + 1, s))
            def _(part=part):
                kv_copy(0, s + 1, s, part).start()

            @pl.when((lax.rem(i + s, n) < second_steps) & (s <= second_steps))
            def _(part=part):
                kv_copy(1, s, s, part).wait_recv()

            @pl.when(kv_moves(1, s + 1, s))
            def _(part=part):
                kv_copy(1, s + 1, s, part).start()

        for direction in (0, 1):

            @pl.when(kv_moves(direction, s, s - 1))
            def _(direction=direction):
                for part in (0, 1):
                    kv_copy(direction, s, s - 1, part).wait_send()

    def w_arrived(copy, s, half, direction, count):
        copy(direction, s, s, half).wait_recv()
        if_step(s < count, lambda: copy(direction, s + 1, s, half).start())

    def to_partner(src, dst, rows_of, send, recv, s):
        pltpu.make_async_remote_copy(
            src_ref=src.at[rows_of],
            dst_ref=dst.at[rows_of],
            send_sem=send,
            recv_sem=recv.at[s - 1],
            device_id={"grp": partner},
            device_id_type=MESH,
        ).start()

    def wait_down(start, stop):
        for d in range(start, stop):
            blocks = int(d <= first_steps) + int(d <= second_steps)
            rest = d_all.at[pl.ds(0, blocks * quarter)]
            pltpu.make_async_copy(rest, rest, dy_recv.at[d - 1]).wait()

    def w_slot(s, half):
        for direction in (0, 1):

            def m_arrived(direction=direction, count=steps_of(direction, True)):
                w_arrived(m_copy, s, half, direction, count)
                to_partner(m_all, o_all, half_of(direction, s, half), y_send, y_recv, s)

            if_step(s <= steps_of(direction, True), m_arrived)
        d = s - BEHIND
        if half == 0 and isinstance(d, int) and d == shared + 1 and shared > 0:
            wait_down(shared, shared + 1)
            for direction in (0, 1):
                if d <= steps_of(direction, False):
                    d_copy(direction, d, shared, 2).start()
        for part in (1,) if half == 0 else (0, 2):
            for direction in (0, 1):

                def d_arrived(direction=direction, part=part, count=steps_of(direction, False)):
                    w_arrived(d_copy, d, part, direction, count)
                    if part == 1 and (not isinstance(d, int) or d <= shared):
                        to_partner(d_all, d_all, d_part(direction, d, 1), dy_send, dy_recv, d)

                if part == 2 and not isinstance(d, int):
                    continue
                if part == 2 and d <= shared:
                    continue
                if_step(both(d > 0, d <= steps_of(direction, False)), d_arrived)

        def d_first():
            for part in (1,) if half == 0 else (0, 2) if shared == 0 else (0,):
                for direction in (0, 1):
                    d_copy(direction, 1, 0, part).start()

        if_step(s == BEHIND, d_first)

    for part in (0, 1):
        for direction in (0, 1):
            pl.when(kv_moves(direction, 1, 0))(kv_copy(direction, 1, 0, part).start)
    for half in (0, 1):
        for direction in (0, 1):
            m_copy(direction, 1, 0, half).start()

    def ow_block(index):
        return ow_all.at[pl.ds(pl.multiple_of(index * width, width), width)]

    def ow_copy(index, where, send, recv):
        return pltpu.make_async_remote_copy(
            src_ref=ow_block(index),
            dst_ref=ow_block(index),
            send_sem=send,
            recv_sem=recv,
            device_id={"tp": where},
            device_id_type=MESH,
        )

    for k in range(2, t, 2):
        ow_copy(c, peer(k), ow_send, ow_recv).start()
    ow_copy(c, sibling, ow_pass_send, ow_pass_recv).start()

    def ow_pass():
        x_rows = ow_all.at[pl.ds(0, (t // 2 - 1) * width)]
        pltpu.make_async_copy(x_rows, x_rows, ow_recv).wait()
        for k in range(2, t, 2):
            ow_copy(peer(k), sibling, ow_pass_send, ow_pass_recv).start()

    scale = width ** (-0.5)

    def terms(block, causal):
        k = kv_all[block, pl.ds(0, tok), :]
        v = kv_all[block, pl.ds(tok, tok), :]
        logit = kv_all[block, pl.ds(2 * tok, 16), :].astype(F32)[0:1, :]
        scores = lax.dot_general(
            q_ref[...], k, (((1,), (1,)), ((), ())), preferred_element_type=F32
        )
        scores = scores * scale + logit
        soft = jnp.log1p(jnp.exp(-jnp.abs(scores)))
        keep = -(jnp.maximum(scores, 0.0) + soft)
        if causal is not None:
            keep = jnp.where(causal, keep, 0.0)
        high = keep.astype(BF16)
        low = (keep - high.astype(F32)).astype(BF16)
        u = upper[...]
        sums = jnp.dot(high, u, preferred_element_type=F32) + jnp.dot(
            low, u, preferred_element_type=F32
        )
        within, total = sums[:, :tile], sums[:, tile:]
        stick = jnp.exp(jnp.minimum(scores, 0.0) - soft + within)
        if causal is not None:
            stick = jnp.where(causal, stick, 0.0)
        part = jnp.dot(stick.astype(BF16), v, preferred_element_type=F32)
        return total, part

    def attend_near(s):
        @pl.when(i >= s)
        def _():
            total, part = terms(i - s, None)
            so_far = run_near[...]
            acc_near[...] += jnp.exp(so_far) * part
            run_near[...] = so_far + total

    def attend_far(s):
        @pl.when((i + s >= n) & (s <= second_steps))
        def _():
            total, part = terms(i + s - n, None)
            acc_far[...] = acc_far[...] * jnp.exp(total) + part

    q_pos = lax.broadcasted_iota(jnp.int32, (tok, tok), 0)
    k_pos = lax.broadcasted_iota(jnp.int32, (tok, tok), 1)
    total, part = terms(i, k_pos < q_pos)
    acc_near[...] = part
    run_near[...] = total

    def group(g, carry):
        s, w = 4 * g, 3 * g
        if t > 2:
            pl.when(g == groups - 1)(ow_pass)
        with jax.named_scope("kv1"):
            kv_slot(s + 1)
        attend_near(s + 1)
        with jax.named_scope("w1a"):
            w_slot(w + 1, 0)
        attend_far(s + 1)
        with jax.named_scope("w1b"):
            w_slot(w + 1, 1)
        with jax.named_scope("kv2"):
            kv_slot(s + 2)
        attend_near(s + 2)
        with jax.named_scope("w2a"):
            w_slot(w + 2, 0)
        attend_far(s + 2)
        with jax.named_scope("kv3"):
            kv_slot(s + 3)
        attend_near(s + 3)
        with jax.named_scope("w2b"):
            w_slot(w + 2, 1)
        attend_far(s + 3)
        with jax.named_scope("w3a"):
            w_slot(w + 3, 0)
        with jax.named_scope("kv4"):
            kv_slot(s + 4)
        attend_near(s + 4)
        with jax.named_scope("w3b"):
            w_slot(w + 3, 1)
        attend_far(s + 4)
        return carry

    lax.fori_loop(0, groups, group, 0)

    def columns(index, size):
        return pl.ds(pl.multiple_of(index * size, size), size)

    def send_attended():
        own = columns(c, width)
        att_all[:, own] = (acc_near[...] + jnp.exp(run_near[...]) * acc_far[...]).astype(BF16)
        for k in range(1, t):
            pltpu.make_async_remote_copy(
                src_ref=att_all.at[:, own],
                dst_ref=att_all.at[:, own],
                send_sem=att_send,
                recv_sem=att_recv,
                device_id={"tp": peer(k)},
                device_id_type=MESH,
            ).start()


    def wait_attended():
        others = att_all.at[:, pl.ds(0, (t - 1) * width)]
        pltpu.make_async_copy(others, others, att_recv).wait()
        passed = ow_all.at[pl.ds(0, (t // 2) * width)]
        pltpu.make_async_copy(passed, passed, ow_pass_recv).wait()

    def project(start, stop):
        def step(j, carry):
            at = columns(j, wide)
            mixed[:, at] = jnp.dot(
                att_all[...], ow_all[:, at], preferred_element_type=F32
            ).astype(BF16)
            return carry

        lax.fori_loop(start, stop, step, 0)

    def normalize(x):
        return x * lax.rsqrt(jnp.mean(x * x, axis=-1, keepdims=True) + EPSILON)

    chunk = 16

    def norms(start, stop):
        def step(j, carry):
            at = columns(j, chunk)
            mid = (
                res_ref[at, :].astype(F32)
                + mix_gain_ref[...] * normalize(mixed[at, :].astype(F32))
            ).astype(BF16)
            middle[at, :] = mid
            normed[at, :] = (ffn_gain_ref[...] * normalize(mid.astype(F32))).astype(BF16)
            return carry

        lax.fori_loop(start, stop, step, 0)

    chunks, per_chunk = d_model // wide, wide // w_rows
    arrived_chunks = max(0, min(chunks, (2 * early + 2 - per_chunk) // per_chunk))
    first_chunk = (i + n - early + per_chunk - 1) // per_chunk

    def act_of(weights, act, start, stop):
        def step(j, carry):
            at = columns(lax.rem(first_chunk + j, chunks), wide)
            act[...] += jnp.dot(normed[:, at], weights[at, :], preferred_element_type=F32)
            return carry

        lax.fori_loop(start, stop, step, 0)

    def wait_other(start, stop):
        for s in range(start, stop):
            blocks = int(s <= first_steps) + int(s <= second_steps)
            rest = o_all.at[pl.ds(0, blocks * w_rows)]
            pltpu.make_async_copy(rest, rest, y_recv.at[s - 1]).wait()

    def hide():
        def step(j, carry):
            at = columns(j, chunk)
            a, b = m_act[at, :], o_act[at, :]
            gate = jnp.where(parity == 0, a, b)
            up = jnp.where(parity == 0, b, a)
            hidden[at, :] = (gate / (1.0 + jnp.exp(-gate)) * up).astype(BF16)
            return carry

        lax.fori_loop(0, tok // chunk, step, 0)

    count, chips = d_model // wide, t // 2
    half_of_rows = tok // 2
    core, chip = lax.rem(c, 2), c // 2

    def rows_at(start, size):
        return pl.ds(pl.multiple_of(start, own_rows), size)

    own_half = rows_at(core * half_of_rows, half_of_rows)
    other_half = rows_at((1 - core) * half_of_rows, half_of_rows)
    in_half = rows_at(chip * own_rows, own_rows)
    own = rows_at(core * half_of_rows + chip * own_rows, own_rows)

    def to_peer(src, dst, send, recv, where):
        pltpu.make_async_remote_copy(
            src_ref=src,
            dst_ref=dst,
            send_sem=send,
            recv_sem=recv,
            device_id={"tp": where},
            device_id_type=MESH,
        ).start()

    def await_all(ref, sem):
        pltpu.make_async_copy(ref, ref, sem).wait()

    whole_at = first_steps - BEHIND
    first_tiles = max(0, min(count, (2 * whole_at + 2 - per_chunk) // per_chunk))
    first_tile = (i + n - whole_at + per_chunk - 1) // per_chunk

    def partial(j, carry):
        p = lax.rem(first_tile + j, count)
        parts[p] = lax.dot_general(
            hidden[...],
            d_all[columns(p, wide), :],
            (((1,), (1,)), ((), ())),
            preferred_element_type=F32,
        ).astype(BF16)
        to_peer(parts.at[p, other_half], core_buf.at[p], cs_send, cs_recv.at[p], sibling)
        return carry

    def between_cores(j, carry):
        p = lax.rem(first_tile + j, count)
        await_all(core_buf.at[p], cs_recv.at[p])
        halves[p] = (parts[p, own_half, :].astype(F32) + core_buf[p].astype(F32)).astype(BF16)
        for far in range(1, chips):
            to = lax.rem(chip + far, chips)
            to_peer(
                halves.at[p, rows_at(to * own_rows, own_rows)],
                rs_buf.at[p, far - 1],
                rs_send,
                rs_recv.at[p],
                2 * to + core,
            )
        return carry

    def between_chips(j, carry):
        p = lax.rem(first_tile + j, count)
        total = halves[p, in_half, :].astype(F32)
        if chips > 1:
            await_all(rs_buf.at[p], rs_recv.at[p])
        for far in range(1, chips):
            total = total + rs_buf[p, far - 1].astype(F32)
        ffn[p, own, :] = total.astype(BF16)
        return p

    def chips_then_cores(j, carry):
        p = between_chips(j, carry)
        for far in range(1, chips):
            to = 2 * lax.rem(chip + far, chips) + core
            to_peer(ffn.at[p, own], ffn.at[p, own], ag_send, ag_recv.at[p], to)
        return carry

    def to_all(p):
        for far in range(1, t):
            to_peer(ffn.at[p, own], ffn.at[p, own], lg_send.at[p], lg_recv.at[p], peer(far))

    def chips_then_all(j, carry):
        to_all(between_chips(j, carry))
        return carry

    def last_partial(j):
        p = lax.rem(first_tile + j, count)
        k = j - (count - LAST)
        parts[p] = lax.dot_general(
            hidden[...],
            d_all[columns(p, wide), :],
            (((1,), (1,)), ((), ())),
            preferred_element_type=F32,
        ).astype(BF16)
        for far in range(1, t):
            to = peer(far)
            start = lax.rem(to, 2) * half_of_rows + to // 2 * own_rows
            to_peer(
                parts.at[p, rows_at(start, own_rows)],
                rs_last.at[k, far - 1],
                ls_send,
                ls_recv.at[k],
                to,
            )

    def last_total(j):
        p = lax.rem(first_tile + j, count)
        k = j - (count - LAST)
        await_all(rs_last.at[k], ls_recv.at[k])
        total = parts[p, own, :].astype(F32)
        for far in range(1, t):
            total = total + rs_last[k, far - 1].astype(F32)
        ffn[p, own, :] = total.astype(BF16)
        to_all(p)

    def to_other_core(j, carry):
        p = lax.rem(first_tile + j, count)
        if chips > 1:
            await_all(rs_buf.at[p], ag_recv.at[p])
        to_peer(ffn.at[p, own_half], ffn.at[p, own_half], cg_send, cg_recv.at[p], sibling)
        return carry

    def zero_acts():
        m_act[...] = jnp.zeros_like(m_act)
        o_act[...] = jnp.zeros_like(o_act)

    n_cols, n_rows = d_model // wide, tok // chunk
    some = arrived_chunks // 2

    def named(name, *bodies):
        def run():
            with jax.named_scope(name):
                for body in bodies:
                    body()

        return run

    tasks = [
        named("zero", zero_acts),
        named("project1", wait_attended, lambda: project(0, n_cols // 2)),
        named("project2", lambda: project(n_cols // 2, n_cols)),
        named("norms1", lambda: norms(0, n_rows // 2)),
        named("norms2", lambda: norms(n_rows // 2, n_rows)),
        named("mine1", lambda: act_of(m_all, m_act, 0, some)),
        named("mine2", lambda: act_of(m_all, m_act, some, arrived_chunks)),
        named(
            "other1",
            lambda: wait_other(1, early + 1),
            lambda: act_of(o_all, o_act, 0, arrived_chunks),
        ),
    ]
    after = [
        named("mine3", lambda: act_of(m_all, m_act, arrived_chunks, chunks)),
        named(
            "other2",
            lambda: wait_other(early + 1, first_steps + 1),
            lambda: act_of(o_all, o_act, arrived_chunks, chunks),
            hide,
            lambda: wait_down(1, shared),
        ),
    ]
    stages = {"partial": partial, "cores": between_cores}
    reached = dict.fromkeys(stages, 0)
    reduced = count - LAST
    near = min(first_tiles, reduced)
    third = (near + 2) // 3
    two = min(2 * third, near)

    def up_to(name, stop):
        def body():
            if reached[name] < stop:
                lax.fori_loop(reached[name], stop, stages[name], 0)
                reached[name] = stop

        return named(name, body)

    after += [
        up_to("partial", third),
        up_to("partial", two),
        lambda: (up_to("partial", near)(), up_to("cores", third)()),
        up_to("cores", two),
    ]
    with jax.named_scope("send_attended"):
        send_attended()
    for s in range(early + 1, first_steps + BEHIND + 1):
        for half in (0, 1):
            with jax.named_scope("wl" if s <= first_steps else "dl"):
                w_slot(s, half)
            if s == first_steps and half == 1:
                while tasks:
                    tasks.pop(0)()
                tasks = after
            elif tasks:
                tasks.pop(0)()
    while tasks:
        tasks.pop(0)()
    up_to("partial", reduced)()
    with jax.named_scope("last_partial"):
        for j in range(reduced, count):
            last_partial(j)
    up_to("cores", reduced)()
    with jax.named_scope("chips"):
        lax.fori_loop(0, two, chips_then_cores, 0)
    with jax.named_scope("last_total"):
        for j in range(reduced, count):
            last_total(j)
    with jax.named_scope("chips_all"):
        lax.fori_loop(two, reduced, chips_then_all, 0)
    with jax.named_scope("back"):
        lax.fori_loop(0, two, to_other_core, 0)

    with jax.named_scope("gathered"):
        for j in range(count):
            p = lax.rem(first_tile + j, count)
            if j < two:
                await_all(core_buf.at[p], cg_recv.at[p])
            else:
                await_all(rs_last.at[0], lg_recv.at[p])

    def finish(j, carry):
        at = columns(j, chunk)
        x = jnp.concatenate([ffn[p, at, :] for p in range(count)], axis=1).astype(F32)
        out[at, :] = (
            middle[at, :].astype(F32) + out_gain_ref[...] * normalize(x)
        ).astype(BF16)
        pltpu.make_async_copy(out.at[at], out_ref.at[at], out_sem).start()
        return carry

    with jax.named_scope("finish"):
        lax.fori_loop(0, tok // chunk, finish, 0)

    def drain(ref, sem):
        pltpu.make_async_copy(ref, ref, sem).wait()

    ring = pl.ds(0, (n - 1) * w_rows)
    drain(m_all.at[ring], m_send)
    drain(m_all.at[ring], y_send)
    over_y = min(shared, first_steps) + min(shared, second_steps)
    d_rows = (n - 1) * w_rows - over_y * quarter
    drain(d_all.at[pl.ds(0, d_rows)], d_send)
    if over_y:
        drain(d_all.at[pl.ds(0, over_y * quarter)], dy_send)
    if t > 2:
        drain(ow_all.at[pl.ds(0, (t // 2 - 1) * width)], ow_send)
    drain(ow_all.at[pl.ds(0, (t // 2) * width)], ow_pass_send)
    drain(att_all.at[:, pl.ds(0, (t - 1) * width)], att_send)
    if reduced:
        drain(core_buf.at[pl.ds(0, reduced)], cs_send)
        if chips > 1:
            drain(rs_buf.at[pl.ds(0, reduced)], rs_send)
    if two:
        drain(core_buf.at[pl.ds(0, two)], cg_send)
        if chips > 1:
            drain(rs_buf.at[pl.ds(0, two)], ag_send)
    drain(rs_last, ls_send)
    for j in range(two, count):
        drain(rs_last.at[0], lg_send.at[lax.rem(first_tile + j, count)])
    pltpu.make_async_copy(out, out_ref, out_sem).wait()


def solution(mesh):
    n, t = mesh.shape["sp"], mesh.shape["tp"]

    def shards(
        query_rows,
        key_rows,
        value_rows,
        key_logit,
        residual,
        out_weight,
        mix_gain,
        ffn_gain,
        out_gain,
        gate_weight,
        up_weight,
        down_weight,
    ):
        tok, width = query_rows.shape
        w_rows, units = gate_weight.shape
        d_model = residual.shape[1]
        tile = 128
        count = d_model // WIDE
        logit = jnp.broadcast_to(key_logit.reshape(1, tok), (16, tok))
        hbm = pl.BlockSpec(memory_space=pltpu.HBM)
        steps = n // 2
        dma = pltpu.SemaphoreType.DMA
        return pl.pallas_call(
            functools.partial(layer_kernel, (n, t)),
            out_shape=jax.ShapeDtypeStruct((tok, d_model), BF16),
            in_specs=[hbm] * 12,
            out_specs=hbm,
            scratch_shapes=[
                pltpu.VMEM((tok, width), BF16),
                pltpu.VMEM((tok, d_model), BF16),
                pltpu.VMEM((1, d_model), F32),
                pltpu.VMEM((1, d_model), F32),
                pltpu.VMEM((1, d_model), F32),
                pltpu.VMEM((n, 2 * tok + 16, width), BF16),
                pltpu.VMEM((n * w_rows, units), BF16),
                pltpu.VMEM((n * w_rows, units), BF16),
                pltpu.VMEM((n * w_rows, units), BF16),
                pltpu.VMEM((t * width, d_model), BF16),
                pltpu.VMEM((tok, t * width), BF16),
                pltpu.VMEM((tok, d_model), BF16),
                pltpu.VMEM((tok, d_model), BF16),
                pltpu.VMEM((tok, d_model), BF16),
                pltpu.VMEM((tok, units), F32),
                pltpu.VMEM((tok, units), F32),
                pltpu.VMEM((tok, units), BF16),
                pltpu.VMEM((count, tok, WIDE), BF16),
                pltpu.VMEM((count, tok // 2, WIDE), BF16),
                pltpu.VMEM((count, tok // 2, WIDE), BF16),
                pltpu.VMEM((count, max(t // 2 - 1, 1), tok // t, WIDE), BF16),
                pltpu.VMEM((count, tok, WIDE), BF16),
                pltpu.VMEM((tile, 2 * tile), BF16),
                pltpu.VMEM((tok, width), F32),
                pltpu.VMEM((tok, width), F32),
                pltpu.VMEM((tok, width), F32),
                dma((12,)),
                dma((2, 2, steps)),
                dma((2, 2, steps)),
                dma,
                dma((2, 2, steps)),
                dma,
                dma((2, 3, steps)),
                dma,
                dma((steps,)),
                dma,
                dma,
                dma,
                dma,
                dma,
                dma,
                dma,
                dma((count,)),
                dma,
                dma((count,)),
                dma,
                dma((count,)),
                dma,
                dma((count,)),
                dma,
                dma((steps,)),
                pltpu.VMEM((tok, d_model), BF16),
                dma,
                pltpu.VMEM((LAST, t - 1, tok // t, WIDE), BF16),
                dma,
                dma((LAST,)),
                dma((count,)),
                dma((count,)),
            ],
            compiler_params=pltpu.CompilerParams(
                collective_id=0, has_side_effects=True, vmem_limit_bytes=67043328
            ),
            name="layer",
        )(
            query_rows,
            key_rows,
            value_rows,
            logit,
            residual,
            out_weight,
            mix_gain.reshape(1, d_model),
            ffn_gain.reshape(1, d_model),
            out_gain.reshape(1, d_model),
            gate_weight,
            up_weight,
            down_weight,
        )

    rows = P(("grp", "sp"), "tp")
    placed = (
        rows,
        rows,
        rows,
        rows,
        P(("grp", "sp"), None),
        P("tp", None),
        P(),
        P(),
        P(),
        P("sp", "tp"),
        P("sp", "tp"),
        P("sp", "tp"),
    )
    return jax.shard_map(
        shards, mesh=mesh, in_specs=placed, out_specs=P(("grp", "sp"), None), check_vma=False
    )
```

```python
import functools

import jax
import jax.numpy as jnp
from jax import lax
from jax.experimental import pallas as pl
from jax.experimental.pallas import tpu as pltpu
from jax.sharding import PartitionSpec as P

EPSILON = 1e-06
MESH = pl.DeviceIdType.MESH
F32 = jnp.float32
BF16 = jnp.bfloat16
WIDE = 256
LOGIT_ROWS = 8
CHUNK = 32
LAST = 2
BEHIND = 2


def layer_kernel(
    sizes,
    q_in,
    k_ref,
    v_ref,
    lg_ref,
    res_in,
    ow_ref,
    mix_gain_in,
    ffn_gain_in,
    out_gain_in,
    gate_ref,
    up_ref,
    down_ref,
    out_ref,
    q_ref,
    res_ref,
    mix_gain_ref,
    ffn_gain_ref,
    out_gain_ref,
    kv_all,
    m_all,
    o_all,
    d_all,
    ow_all,
    att_all,
    mixed,
    middle,
    normed,
    m_act,
    o_act,
    hidden,
    parts,
    core_buf,
    halves,
    rs_buf,
    ffn,
    upper,
    acc_near,
    run_near,
    acc_far,
    local_sem,
    kv_send,
    kv_recv,
    m_send,
    m_recv,
    d_send,
    d_recv,
    y_send,
    y_recv,
    ow_send,
    ow_recv,
    ow_pass_send,
    ow_pass_recv,
    att_send,
    att_recv,
    rs_send,
    rs_recv,
    ag_send,
    ag_recv,
    cs_send,
    cs_recv,
    cg_send,
    cg_recv,
    dy_send,
    dy_recv,
    out,
    out_sem,
    rs_last,
    ls_send,
    ls_recv,
    lg_send,
    lg_recv,
):
    n, t = sizes
    tok, width = q_in.shape
    w_rows = gate_ref.shape[0]
    half_rows = w_rows // 2
    d_model = res_ref.shape[1]
    first_steps, second_steps = n // 2, n - 1 - n // 2
    tile, wide = 128, WIDE
    own_rows = tok // t
    grp, i, c = lax.axis_index("grp"), lax.axis_index("sp"), lax.axis_index("tp")
    parity = lax.rem(grp, 2)
    partner = grp + 1 - 2 * parity
    sibling = c + 1 - 2 * lax.rem(c, 2)
    right, left = lax.rem(i + 1, n), lax.rem(i + n - 1, n)

    def peer(k):
        return lax.rem(c + k, t)

    kv_own = kv_all.at[i]
    w_own = pl.ds(pl.multiple_of(i * w_rows, w_rows), w_rows)
    copies = [
        pltpu.make_async_copy(k_ref, kv_own.at[pl.ds(0, tok)], local_sem.at[0]),
        pltpu.make_async_copy(v_ref, kv_own.at[pl.ds(tok, tok)], local_sem.at[1]),
        pltpu.make_async_copy(lg_ref, kv_own.at[pl.ds(2 * tok, LOGIT_ROWS)], local_sem.at[2]),
        pltpu.make_async_copy(down_ref, d_all.at[w_own], local_sem.at[3]),
        pltpu.make_async_copy(
            ow_ref, ow_all.at[pl.ds(pl.multiple_of(c * width, width), width)], local_sem.at[4]
        ),
        pltpu.make_async_copy(q_in, q_ref, local_sem.at[7]),
        pltpu.make_async_copy(res_in, res_ref, local_sem.at[8]),
        pltpu.make_async_copy(mix_gain_in, mix_gain_ref, local_sem.at[9]),
        pltpu.make_async_copy(ffn_gain_in, ffn_gain_ref, local_sem.at[10]),
        pltpu.make_async_copy(out_gain_in, out_gain_ref, local_sem.at[11]),
    ]
    for copy in copies:
        copy.start()

    @pl.when(parity == 0)
    def _():
        pltpu.make_async_copy(gate_ref, m_all.at[w_own], local_sem.at[5]).start()
        pltpu.make_async_copy(up_ref, o_all.at[w_own], local_sem.at[6]).start()

    @pl.when(parity == 1)
    def _():
        pltpu.make_async_copy(up_ref, m_all.at[w_own], local_sem.at[5]).start()
        pltpu.make_async_copy(gate_ref, o_all.at[w_own], local_sem.at[6]).start()

    barrier = pltpu.get_barrier_semaphore()
    for where in [{"sp": right}, {"sp": left}, {"grp": partner}] + [
        {"tp": peer(k)} for k in range(1, t)
    ]:
        pl.semaphore_signal(barrier, inc=1, device_id=where, device_id_type=MESH)

    rows = lax.broadcasted_iota(jnp.int32, (tile, 2 * tile), 0)
    cols = lax.broadcasted_iota(jnp.int32, (tile, 2 * tile), 1)
    upper[...] = jnp.where((rows > cols) | (cols >= tile), 1.0, 0.0).astype(BF16)
    acc_far[...] = jnp.zeros_like(acc_far)

    with jax.named_scope("local"):
        for copy in copies:
            copy.wait()
        pltpu.make_async_copy(gate_ref, m_all.at[w_own], local_sem.at[5]).wait()
        pltpu.make_async_copy(up_ref, o_all.at[w_own], local_sem.at[6]).wait()
    with jax.named_scope("barrier"):
        pl.semaphore_wait(barrier, t + 2)

    def block_at(direction, back):
        return lax.rem(i + n - back, n) if direction == 0 else lax.rem(i + back, n)

    def turn(step, turns):
        return (step - 1) % turns if isinstance(step, int) else lax.rem(step - 1, turns)

    def kv_copy(direction, step, back, part):
        rows_of = pl.ds(0, tok) if part == 0 else pl.ds(tok, tok + LOGIT_ROWS)
        block = kv_all.at[block_at(direction, back), rows_of]
        return pltpu.make_async_remote_copy(
            src_ref=block,
            dst_ref=block,
            send_sem=kv_send.at[direction, part, turn(step, 2)],
            recv_sem=kv_recv.at[direction, part, turn(step, 8)],
            device_id={"sp": right if direction == 0 else left},
            device_id_type=MESH,
        )

    def half_of(direction, back, half):
        start = block_at(direction, back) * w_rows + half * half_rows
        return pl.ds(pl.multiple_of(start, half_rows), half_rows)

    quarter = half_rows // 2
    groups = first_steps // 4
    early = 3 * groups
    shared = max(0, early - BEHIND)

    def d_part(direction, back, part):
        if part == 0:
            return half_of(direction, back, 0)
        which = parity if part == 1 else 1 - parity
        start = block_at(direction, back) * w_rows + half_rows + which * quarter
        return pl.ds(pl.multiple_of(start, quarter), quarter)

    def w_copy(ref, send, recv, direction, step, half, rows_of):
        part = ref.at[rows_of]
        return pltpu.make_async_remote_copy(
            src_ref=part,
            dst_ref=part,
            send_sem=send,
            recv_sem=recv.at[direction, half, turn(step, 4)],
            device_id={"sp": right if direction == 0 else left},
            device_id_type=MESH,
        )

    def m_copy(direction, step, back, half):
        return w_copy(m_all, m_send, m_recv, direction, step, half, half_of(direction, back, half))

    def d_copy(direction, step, back, half):
        return w_copy(d_all, d_send, d_recv, direction, step, half, d_part(direction, back, half))

    def steps_of(direction, flipped):
        return first_steps if direction == int(flipped) else second_steps

    def if_step(condition, body):
        if isinstance(condition, bool):
            if condition:
                body()
        else:
            pl.when(condition)(body)

    def both(a, b):
        return (a and b) if isinstance(a, bool) else a & b

    def kv_moves(direction, step, back):
        if direction == 0:
            return (i >= back) & (i < n - 1) & (step <= first_steps)
        return (lax.rem(i + back, n) < second_steps) & (step <= second_steps)

    def kv_slot(s):
        for part in (0, 1):

            @pl.when((i >= s) & (s <= first_steps))
            def _(part=part):
                kv_copy(0, s, s, part).wait_recv()

            @pl.when(kv_moves(0, s + 1, s))
            def _(part=part):
                kv_copy(0, s + 1, s, part).start()

            @pl.when((lax.rem(i + s, n) < second_steps) & (s <= second_steps))
            def _(part=part):
                kv_copy(1, s, s, part).wait_recv()

            @pl.when(kv_moves(1, s + 1, s))
            def _(part=part):
                kv_copy(1, s + 1, s, part).start()

        for direction in (0, 1):

            @pl.when(kv_moves(direction, s, s - 1))
            def _(direction=direction):
                for part in (0, 1):
                    kv_copy(direction, s, s - 1, part).wait_send()

    def w_arrived(copy, s, half, direction, count):
        copy(direction, s, s, half).wait_recv()
        if_step(s < count, lambda: copy(direction, s + 1, s, half).start())

    def to_partner(src, dst, rows_of, send, recv):
        pltpu.make_async_remote_copy(
            src_ref=src.at[rows_of],
            dst_ref=dst.at[rows_of],
            send_sem=send,
            recv_sem=recv,
            device_id={"grp": partner},
            device_id_type=MESH,
        ).start()

    def wait_down(start, stop, which):
        blocks = min(stop - 1, first_steps) + min(stop - 1, second_steps)
        blocks -= min(start - 1, first_steps) + min(start - 1, second_steps)
        if blocks > 0:
            rest = d_all.at[pl.ds(0, blocks * quarter)]
            pltpu.make_async_copy(rest, rest, dy_recv.at[which]).wait()

    def w_slot(s, half):
        d = s - BEHIND

        def m_parts():
            for direction in (0, 1):

                def m_arrived(direction=direction, count=steps_of(direction, True)):
                    w_arrived(m_copy, s, half, direction, count)
                    y_sem = y_recv.at[0 if not isinstance(s, int) or s <= early else 1]
                    to_partner(m_all, o_all, half_of(direction, s, half), y_send, y_sem)

                if_step(s <= steps_of(direction, True), m_arrived)
        def d_parts():
            if half == 0 and isinstance(d, int) and d == shared + 1 and shared > 0:
                wait_down(shared, shared + 1, 1)
                for direction in (0, 1):
                    if d <= steps_of(direction, False):
                        d_copy(direction, d, shared, 2).start()
            for part in (1,) if half == 0 else (0, 2):
                for direction in (0, 1):

                    def d_arrived(direction=direction, part=part, count=steps_of(direction, False)):
                        w_arrived(d_copy, d, part, direction, count)
                        if part == 1 and (not isinstance(d, int) or d <= shared):
                            dy_sem = dy_recv.at[int(d == shared) if isinstance(d, int) else (d == shared).astype(jnp.int32)]
                            to_partner(d_all, d_all, d_part(direction, d, 1), dy_send, dy_sem)

                    if part == 2 and not isinstance(d, int):
                        continue
                    if part == 2 and d <= shared:
                        continue
                    if_step(both(d > 0, d <= steps_of(direction, False)), d_arrived)

        for body in (d_parts, m_parts) if half == 0 else (m_parts, d_parts):
            body()

        def d_first():
            for part in (1,) if half == 0 else (0, 2) if shared == 0 else (0,):
                for direction in (0, 1):
                    d_copy(direction, 1, 0, part).start()

        if_step(s == BEHIND, d_first)

    for part in (0, 1):
        for direction in (0, 1):
            pl.when(kv_moves(direction, 1, 0))(kv_copy(direction, 1, 0, part).start)
    for half in (0, 1):
        for direction in (0, 1):
            m_copy(direction, 1, 0, half).start()

    def ow_block(index):
        return ow_all.at[pl.ds(pl.multiple_of(index * width, width), width)]

    def ow_copy(index, where, send, recv):
        return pltpu.make_async_remote_copy(
            src_ref=ow_block(index),
            dst_ref=ow_block(index),
            send_sem=send,
            recv_sem=recv,
            device_id={"tp": where},
            device_id_type=MESH,
        )

    for k in range(2, t, 2):
        ow_copy(c, peer(k), ow_send, ow_recv).start()
    ow_copy(c, sibling, ow_pass_send, ow_pass_recv).start()

    def ow_pass():
        x_rows = ow_all.at[pl.ds(0, (t // 2 - 1) * width)]
        pltpu.make_async_copy(x_rows, x_rows, ow_recv).wait()
        for k in range(2, t, 2):
            ow_copy(peer(k), sibling, ow_pass_send, ow_pass_recv).start()

    scale = width ** (-0.5)

    def terms(block, causal):
        k = kv_all[block, pl.ds(0, tok), :]
        v = kv_all[block, pl.ds(tok, tok), :]
        logit = kv_all[block, pl.ds(2 * tok, LOGIT_ROWS), :].astype(F32)[0:1, :]
        scores = lax.dot_general(
            q_ref[...], k, (((1,), (1,)), ((), ())), preferred_element_type=F32
        )
        scores = scores * scale + logit
        soft = jnp.log1p(jnp.exp(-jnp.abs(scores)))
        keep = -(jnp.maximum(scores, 0.0) + soft)
        if causal is not None:
            keep = jnp.where(causal, keep, 0.0)
        high = keep.astype(BF16)
        low = (keep - high.astype(F32)).astype(BF16)
        u = upper[...]
        sums = jnp.dot(high, u, preferred_element_type=F32) + jnp.dot(
            low, u, preferred_element_type=F32
        )
        within, total = sums[:, :tile], sums[:, tile:]
        stick = jnp.exp(jnp.minimum(scores, 0.0) - soft + within)
        if causal is not None:
            stick = jnp.where(causal, stick, 0.0)
        part = jnp.dot(stick.astype(BF16), v, preferred_element_type=F32)
        return total, part

    def attend_near(s):
        @pl.when(i >= s)
        def _():
            total, part = terms(i - s, None)
            so_far = run_near[...]
            acc_near[...] += jnp.exp(so_far) * part
            run_near[...] = so_far + total

    def attend_far(s):
        @pl.when((i + s >= n) & (s <= second_steps))
        def _():
            total, part = terms(i + s - n, None)
            acc_far[...] = acc_far[...] * jnp.exp(total) + part

    q_pos = lax.broadcasted_iota(jnp.int32, (tok, tok), 0)
    k_pos = lax.broadcasted_iota(jnp.int32, (tok, tok), 1)
    total, part = terms(i, k_pos < q_pos)
    acc_near[...] = part
    run_near[...] = total

    def group(g, carry):
        s, w = 4 * g, 3 * g
        if t > 2:
            pl.when(g == groups - 1)(ow_pass)
        with jax.named_scope("kv1"):
            kv_slot(s + 1)
        attend_near(s + 1)
        with jax.named_scope("w1a"):
            w_slot(w + 1, 0)
        attend_far(s + 1)
        with jax.named_scope("w1b"):
            w_slot(w + 1, 1)
        with jax.named_scope("kv2"):
            kv_slot(s + 2)
        attend_near(s + 2)
        with jax.named_scope("w2a"):
            w_slot(w + 2, 0)
        attend_far(s + 2)
        with jax.named_scope("kv3"):
            kv_slot(s + 3)
        attend_near(s + 3)
        with jax.named_scope("w2b"):
            w_slot(w + 2, 1)
        attend_far(s + 3)
        with jax.named_scope("w3a"):
            w_slot(w + 3, 0)
        with jax.named_scope("kv4"):
            kv_slot(s + 4)
        attend_near(s + 4)
        with jax.named_scope("w3b"):
            w_slot(w + 3, 1)
        attend_far(s + 4)
        return carry

    lax.fori_loop(0, groups, group, 0)

    def columns(index, size):
        return pl.ds(pl.multiple_of(index * size, size), size)

    def send_attended():
        own = columns(c, width)
        att_all[:, own] = (acc_near[...] + jnp.exp(run_near[...]) * acc_far[...]).astype(BF16)
        for k in range(1, t):
            pltpu.make_async_remote_copy(
                src_ref=att_all.at[:, own],
                dst_ref=att_all.at[:, own],
                send_sem=att_send,
                recv_sem=att_recv,
                device_id={"tp": peer(k)},
                device_id_type=MESH,
            ).start()


    def wait_attended():
        others = att_all.at[:, pl.ds(0, (t - 1) * width)]
        pltpu.make_async_copy(others, others, att_recv).wait()
        passed = ow_all.at[pl.ds(0, (t // 2) * width)]
        pltpu.make_async_copy(passed, passed, ow_pass_recv).wait()

    def project(start, stop):
        def step(j, carry):
            at = columns(j, wide)
            mixed[:, at] = jnp.dot(
                att_all[...], ow_all[:, at], preferred_element_type=F32
            ).astype(BF16)
            return carry

        lax.fori_loop(start, stop, step, 0)

    def normalize(x):
        return x * lax.rsqrt(jnp.mean(x * x, axis=-1, keepdims=True) + EPSILON)

    chunk = CHUNK

    def norms(start, stop):
        def step(j, carry):
            at = columns(j, chunk)
            mid = (
                res_ref[at, :].astype(F32)
                + mix_gain_ref[...] * normalize(mixed[at, :].astype(F32))
            ).astype(BF16)
            middle[at, :] = mid
            normed[at, :] = (ffn_gain_ref[...] * normalize(mid.astype(F32))).astype(BF16)
            return carry

        lax.fori_loop(start, stop, step, 0)

    chunks, per_chunk = d_model // wide, wide // w_rows
    arrived_chunks = max(0, min(chunks, (2 * early + 2 - per_chunk) // per_chunk))
    first_chunk = (i + n - early + per_chunk - 1) // per_chunk

    def act_of(weights, act, start, stop):
        def step(j, carry):
            at = columns(lax.rem(first_chunk + j, chunks), wide)
            act[...] += jnp.dot(normed[:, at], weights[at, :], preferred_element_type=F32)
            return carry

        lax.fori_loop(start, stop, step, 0)

    def wait_other(start, stop, which):
        blocks = min(stop - 1, first_steps) + min(stop - 1, second_steps)
        blocks -= min(start - 1, first_steps) + min(start - 1, second_steps)
        if blocks:
            rest = o_all.at[pl.ds(0, blocks * w_rows)]
            pltpu.make_async_copy(rest, rest, y_recv.at[which]).wait()

    def hide():
        def step(j, carry):
            at = columns(j, chunk)
            a, b = m_act[at, :], o_act[at, :]
            gate = jnp.where(parity == 0, a, b)
            up = jnp.where(parity == 0, b, a)
            hidden[at, :] = (gate / (1.0 + jnp.exp(-gate)) * up).astype(BF16)
            return carry

        lax.fori_loop(0, tok // chunk, step, 0)

    count, chips = d_model // wide, t // 2
    half_of_rows = tok // 2
    core, chip = lax.rem(c, 2), c // 2

    def rows_at(start, size):
        return pl.ds(pl.multiple_of(start, own_rows), size)

    own_half = rows_at(core * half_of_rows, half_of_rows)
    other_half = rows_at((1 - core) * half_of_rows, half_of_rows)
    in_half = rows_at(chip * own_rows, own_rows)
    own = rows_at(core * half_of_rows + chip * own_rows, own_rows)

    def to_peer(src, dst, send, recv, where):
        pltpu.make_async_remote_copy(
            src_ref=src,
            dst_ref=dst,
            send_sem=send,
            recv_sem=recv,
            device_id={"tp": where},
            device_id_type=MESH,
        ).start()

    def await_all(ref, sem):
        pltpu.make_async_copy(ref, ref, sem).wait()

    whole_at = first_steps - BEHIND
    first_tiles = max(0, min(count, (2 * whole_at + 2 - per_chunk) // per_chunk))
    first_tile = (i + n - whole_at + per_chunk - 1) // per_chunk

    def partial(j, carry):
        p = lax.rem(first_tile + j, count)
        parts[p] = lax.dot_general(
            hidden[...],
            d_all[columns(p, wide), :],
            (((1,), (1,)), ((), ())),
            preferred_element_type=F32,
        ).astype(BF16)
        to_peer(parts.at[p, other_half], core_buf.at[p], cs_send, cs_recv.at[p], sibling)
        return carry

    def between_cores(j, carry):
        p = lax.rem(first_tile + j, count)
        await_all(core_buf.at[p], cs_recv.at[p])
        halves[p] = (parts[p, own_half, :].astype(F32) + core_buf[p].astype(F32)).astype(BF16)
        for far in range(1, chips):
            to = lax.rem(chip + far, chips)
            to_peer(
                halves.at[p, rows_at(to * own_rows, own_rows)],
                rs_buf.at[p, far - 1],
                rs_send,
                rs_recv.at[p],
                2 * to + core,
            )
        return carry

    def between_chips(j, carry):
        p = lax.rem(first_tile + j, count)
        total = halves[p, in_half, :].astype(F32)
        if chips > 1:
            await_all(rs_buf.at[p], rs_recv.at[p])
        for far in range(1, chips):
            total = total + rs_buf[p, far - 1].astype(F32)
        ffn[p, own, :] = total.astype(BF16)
        return p

    def chips_then_cores(j, carry):
        p = between_chips(j, carry)
        for far in range(1, chips):
            to = 2 * lax.rem(chip + far, chips) + core
            to_peer(ffn.at[p, own], ffn.at[p, own], ag_send, ag_recv.at[p], to)
        return carry

    def to_all(p):
        for far in range(1, t):
            to_peer(ffn.at[p, own], ffn.at[p, own], lg_send.at[p], lg_recv.at[p], peer(far))

    def chips_then_all(j, carry):
        to_all(between_chips(j, carry))
        return carry

    def last_partial(j):
        p = lax.rem(first_tile + j, count)
        k = j - (count - LAST)
        parts[p] = lax.dot_general(
            hidden[...],
            d_all[columns(p, wide), :],
            (((1,), (1,)), ((), ())),
            preferred_element_type=F32,
        ).astype(BF16)
        for far in range(1, t):
            to = peer(far)
            start = lax.rem(to, 2) * half_of_rows + to // 2 * own_rows
            to_peer(
                parts.at[p, rows_at(start, own_rows)],
                rs_last.at[k, far - 1],
                ls_send,
                ls_recv.at[k],
                to,
            )

    def last_total(j):
        p = lax.rem(first_tile + j, count)
        k = j - (count - LAST)
        await_all(rs_last.at[k], ls_recv.at[k])
        total = parts[p, own, :].astype(F32)
        for far in range(1, t):
            total = total + rs_last[k, far - 1].astype(F32)
        ffn[p, own, :] = total.astype(BF16)
        to_all(p)

    def to_other_core(j, carry):
        p = lax.rem(first_tile + j, count)
        if chips > 1:
            await_all(rs_buf.at[p], ag_recv.at[p])
        to_peer(ffn.at[p, own_half], ffn.at[p, own_half], cg_send, cg_recv.at[p], sibling)
        return carry

    def zero_acts():
        m_act[...] = jnp.zeros_like(m_act)
        o_act[...] = jnp.zeros_like(o_act)

    n_cols, n_rows = d_model // wide, tok // chunk
    some = arrived_chunks // 2

    def named(name, *bodies):
        def run():
            with jax.named_scope(name):
                for body in bodies:
                    body()

        return run

    tasks = [
        named("zero", zero_acts),
        named("project1", wait_attended, lambda: project(0, n_cols // 2)),
        named("project2", lambda: project(n_cols // 2, n_cols)),
        named("norms1", lambda: norms(0, n_rows // 2)),
        named("norms2", lambda: norms(n_rows // 2, n_rows)),
        named("mine1", lambda: act_of(m_all, m_act, 0, some)),
        named("mine2", lambda: act_of(m_all, m_act, some, arrived_chunks)),
        named(
            "other1",
            lambda: wait_other(1, early + 1, 0),
            lambda: act_of(o_all, o_act, 0, arrived_chunks),
        ),
    ]
    after = [
        named("mine3", lambda: act_of(m_all, m_act, arrived_chunks, chunks)),
        named(
            "other2",
            lambda: wait_other(early + 1, first_steps + 1, 1),
            lambda: act_of(o_all, o_act, arrived_chunks, chunks),
            hide,
            lambda: wait_down(1, shared, 0),
        ),
    ]
    stages = {"partial": partial, "cores": between_cores}
    reached = dict.fromkeys(stages, 0)
    reduced = count - LAST
    near = min(first_tiles, reduced)
    third = (near + 2) // 3
    two = min(2 * third, near)

    def up_to(name, stop):
        def body():
            if reached[name] < stop:
                lax.fori_loop(reached[name], stop, stages[name], 0)
                reached[name] = stop

        return named(name, body)

    after += [
        up_to("partial", third),
        up_to("partial", two),
        lambda: (up_to("partial", near)(), up_to("cores", third)()),
        up_to("cores", two),
    ]
    with jax.named_scope("send_attended"):
        send_attended()
    for s in range(early + 1, first_steps + BEHIND + 1):
        for half in (0, 1):
            with jax.named_scope("wl" if s <= first_steps else "dl"):
                w_slot(s, half)
            if s == first_steps and half == 1:
                while tasks:
                    tasks.pop(0)()
                tasks = after
            elif tasks:
                tasks.pop(0)()
    while tasks:
        tasks.pop(0)()
    up_to("partial", reduced)()
    with jax.named_scope("last_partial"):
        for j in range(reduced, count):
            last_partial(j)
    up_to("cores", reduced)()
    with jax.named_scope("chips"):
        lax.fori_loop(0, two, chips_then_cores, 0)
    with jax.named_scope("last_total"):
        for j in range(reduced, count):
            last_total(j)
    with jax.named_scope("chips_all"):
        lax.fori_loop(two, reduced, chips_then_all, 0)
    with jax.named_scope("back"):
        lax.fori_loop(0, two, to_other_core, 0)

    with jax.named_scope("gathered"):
        for j in range(count):
            p = lax.rem(first_tile + j, count)
            if j < two:
                await_all(core_buf.at[p], cg_recv.at[p])
            else:
                await_all(rs_last.at[0], lg_recv.at[p])

    def finish(j, carry):
        at = columns(j, chunk)
        x = jnp.concatenate([ffn[p, at, :] for p in range(count)], axis=1).astype(F32)
        out[at, :] = (
            middle[at, :].astype(F32) + out_gain_ref[...] * normalize(x)
        ).astype(BF16)
        pltpu.make_async_copy(out.at[at], out_ref.at[at], out_sem).start()
        return carry

    with jax.named_scope("finish"):
        lax.fori_loop(0, tok // chunk, finish, 0)

    def drain(ref, sem):
        pltpu.make_async_copy(ref, ref, sem).wait()

    ring = pl.ds(0, (n - 1) * w_rows)
    drain(m_all.at[ring], m_send)
    drain(m_all.at[ring], y_send)
    over_y = min(shared, first_steps) + min(shared, second_steps)
    d_rows = (n - 1) * w_rows - over_y * quarter
    drain(d_all.at[pl.ds(0, d_rows)], d_send)
    if over_y:
        drain(d_all.at[pl.ds(0, over_y * quarter)], dy_send)
    if t > 2:
        drain(ow_all.at[pl.ds(0, (t // 2 - 1) * width)], ow_send)
    drain(ow_all.at[pl.ds(0, (t // 2) * width)], ow_pass_send)
    drain(att_all.at[:, pl.ds(0, (t - 1) * width)], att_send)
    if reduced:
        drain(core_buf.at[pl.ds(0, reduced)], cs_send)
        if chips > 1:
            drain(rs_buf.at[pl.ds(0, reduced)], rs_send)
    if two:
        drain(core_buf.at[pl.ds(0, two)], cg_send)
        if chips > 1:
            drain(rs_buf.at[pl.ds(0, two)], ag_send)
    drain(rs_last, ls_send)
    for j in range(two, count):
        drain(rs_last.at[0], lg_send.at[lax.rem(first_tile + j, count)])
    pltpu.make_async_copy(out, out_ref, out_sem).wait()


def solution(mesh):
    n, t = mesh.shape["sp"], mesh.shape["tp"]

    def shards(
        query_rows,
        key_rows,
        value_rows,
        key_logit,
        residual,
        out_weight,
        mix_gain,
        ffn_gain,
        out_gain,
        gate_weight,
        up_weight,
        down_weight,
    ):
        tok, width = query_rows.shape
        w_rows, units = gate_weight.shape
        d_model = residual.shape[1]
        tile = 128
        count = d_model // WIDE
        logit = jnp.broadcast_to(key_logit.reshape(1, tok), (LOGIT_ROWS, tok))
        hbm = pl.BlockSpec(memory_space=pltpu.HBM)
        dma = pltpu.SemaphoreType.DMA
        return pl.pallas_call(
            functools.partial(layer_kernel, (n, t)),
            out_shape=jax.ShapeDtypeStruct((tok, d_model), BF16),
            in_specs=[hbm] * 12,
            out_specs=hbm,
            scratch_shapes=[
                pltpu.VMEM((tok, width), BF16),
                pltpu.VMEM((tok, d_model), BF16),
                pltpu.VMEM((1, d_model), F32),
                pltpu.VMEM((1, d_model), F32),
                pltpu.VMEM((1, d_model), F32),
                pltpu.VMEM((n, 2 * tok + LOGIT_ROWS, width), BF16),
                pltpu.VMEM((n * w_rows, units), BF16),
                pltpu.VMEM((n * w_rows, units), BF16),
                pltpu.VMEM((n * w_rows, units), BF16),
                pltpu.VMEM((t * width, d_model), BF16),
                pltpu.VMEM((tok, t * width), BF16),
                pltpu.VMEM((tok, d_model), BF16),
                pltpu.VMEM((tok, d_model), BF16),
                pltpu.VMEM((tok, d_model), BF16),
                pltpu.VMEM((tok, units), F32),
                pltpu.VMEM((tok, units), F32),
                pltpu.VMEM((tok, units), BF16),
                pltpu.VMEM((count, tok, WIDE), BF16),
                pltpu.VMEM((count, tok // 2, WIDE), BF16),
                pltpu.VMEM((count, tok // 2, WIDE), BF16),
                pltpu.VMEM((count, max(t // 2 - 1, 1), tok // t, WIDE), BF16),
                pltpu.VMEM((count, tok, WIDE), BF16),
                pltpu.VMEM((tile, 2 * tile), BF16),
                pltpu.VMEM((tok, width), F32),
                pltpu.VMEM((tok, width), F32),
                pltpu.VMEM((tok, width), F32),
                dma((12,)),
                dma((2, 2, 2)),
                dma((2, 2, 8)),
                dma,
                dma((2, 2, 4)),
                dma,
                dma((2, 3, 4)),
                dma,
                dma((2,)),
                dma,
                dma,
                dma,
                dma,
                dma,
                dma,
                dma,
                dma((count,)),
                dma,
                dma((count,)),
                dma,
                dma((count,)),
                dma,
                dma((count,)),
                dma,
                dma((2,)),
                pltpu.VMEM((tok, d_model), BF16),
                dma,
                pltpu.VMEM((LAST, t - 1, tok // t, WIDE), BF16),
                dma,
                dma((LAST,)),
                dma((count,)),
                dma((count,)),
            ],
            compiler_params=pltpu.CompilerParams(
                collective_id=0, has_side_effects=True, vmem_limit_bytes=67043328
            ),
            name="layer",
        )(
            query_rows,
            key_rows,
            value_rows,
            logit,
            residual,
            out_weight,
            mix_gain.reshape(1, d_model),
            ffn_gain.reshape(1, d_model),
            out_gain.reshape(1, d_model),
            gate_weight,
            up_weight,
            down_weight,
        )

    rows = P(("grp", "sp"), "tp")
    placed = (
        rows,
        rows,
        rows,
        rows,
        P(("grp", "sp"), None),
        P("tp", None),
        P(),
        P(),
        P(),
        P("sp", "tp"),
        P("sp", "tp"),
        P("sp", "tp"),
    )
    return jax.shard_map(
        shards, mesh=mesh, in_specs=placed, out_specs=P(("grp", "sp"), None), check_vma=False
    )
```

```python
import functools

import jax
import jax.numpy as jnp
from jax import lax
from jax.experimental import pallas as pl
from jax.experimental.pallas import tpu as pltpu
from jax.sharding import PartitionSpec as P

EPSILON = 1e-06
MESH = pl.DeviceIdType.MESH
F32 = jnp.float32
BF16 = jnp.bfloat16
WIDE = 256
LOGIT_ROWS = 8
CHUNK = 32
LAST = 2
BEHIND = 1


def layer_kernel(
    sizes,
    q_in,
    k_ref,
    v_ref,
    lg_ref,
    res_in,
    ow_ref,
    mix_gain_in,
    ffn_gain_in,
    out_gain_in,
    gate_ref,
    up_ref,
    down_ref,
    out_ref,
    q_ref,
    res_ref,
    mix_gain_ref,
    ffn_gain_ref,
    out_gain_ref,
    kv_all,
    m_all,
    o_all,
    d_all,
    ow_all,
    att_all,
    mixed,
    middle,
    normed,
    m_act,
    o_act,
    hidden,
    parts,
    core_buf,
    halves,
    rs_buf,
    ffn,
    upper,
    acc_near,
    run_near,
    acc_far,
    local_sem,
    kv_send,
    kv_recv,
    m_send,
    m_recv,
    d_send,
    d_recv,
    y_send,
    y_recv,
    ow_send,
    ow_recv,
    ow_pass_send,
    ow_pass_recv,
    att_send,
    att_recv,
    rs_send,
    rs_recv,
    ag_send,
    ag_recv,
    cs_send,
    cs_recv,
    cg_send,
    cg_recv,
    dy_send,
    dy_recv,
    out,
    out_sem,
    rs_last,
    ls_send,
    ls_recv,
    lg_send,
    lg_recv,
):
    n, t = sizes
    tok, width = q_in.shape
    w_rows = gate_ref.shape[0]
    half_rows = w_rows // 2
    d_model = res_ref.shape[1]
    first_steps, second_steps = n // 2, n - 1 - n // 2
    tile, wide = 128, WIDE
    own_rows = tok // t
    grp, i, c = lax.axis_index("grp"), lax.axis_index("sp"), lax.axis_index("tp")
    parity = lax.rem(grp, 2)
    partner = grp + 1 - 2 * parity
    sibling = c + 1 - 2 * lax.rem(c, 2)
    right, left = lax.rem(i + 1, n), lax.rem(i + n - 1, n)

    def peer(k):
        return lax.rem(c + k, t)

    kv_own = kv_all.at[i]
    w_own = pl.ds(pl.multiple_of(i * w_rows, w_rows), w_rows)
    copies = [
        pltpu.make_async_copy(k_ref, kv_own.at[pl.ds(0, tok)], local_sem.at[0]),
        pltpu.make_async_copy(v_ref, kv_own.at[pl.ds(tok, tok)], local_sem.at[1]),
        pltpu.make_async_copy(lg_ref, kv_own.at[pl.ds(2 * tok, LOGIT_ROWS)], local_sem.at[2]),
        pltpu.make_async_copy(down_ref, d_all.at[w_own], local_sem.at[3]),
        pltpu.make_async_copy(
            ow_ref, ow_all.at[pl.ds(pl.multiple_of(c * width, width), width)], local_sem.at[4]
        ),
        pltpu.make_async_copy(q_in, q_ref, local_sem.at[7]),
        pltpu.make_async_copy(res_in, res_ref, local_sem.at[8]),
        pltpu.make_async_copy(mix_gain_in, mix_gain_ref, local_sem.at[9]),
        pltpu.make_async_copy(ffn_gain_in, ffn_gain_ref, local_sem.at[10]),
        pltpu.make_async_copy(out_gain_in, out_gain_ref, local_sem.at[11]),
    ]
    for copy in copies:
        copy.start()

    @pl.when(parity == 0)
    def _():
        pltpu.make_async_copy(gate_ref, m_all.at[w_own], local_sem.at[5]).start()
        pltpu.make_async_copy(up_ref, o_all.at[w_own], local_sem.at[6]).start()

    @pl.when(parity == 1)
    def _():
        pltpu.make_async_copy(up_ref, m_all.at[w_own], local_sem.at[5]).start()
        pltpu.make_async_copy(gate_ref, o_all.at[w_own], local_sem.at[6]).start()

    barrier = pltpu.get_barrier_semaphore()
    for where in [{"sp": right}, {"sp": left}, {"grp": partner}] + [
        {"tp": peer(k)} for k in range(1, t)
    ]:
        pl.semaphore_signal(barrier, inc=1, device_id=where, device_id_type=MESH)

    rows = lax.broadcasted_iota(jnp.int32, (tile, 2 * tile), 0)
    cols = lax.broadcasted_iota(jnp.int32, (tile, 2 * tile), 1)
    upper[...] = jnp.where((rows > cols) | (cols >= tile), 1.0, 0.0).astype(BF16)
    acc_far[...] = jnp.zeros_like(acc_far)

    with jax.named_scope("local"):
        for copy in copies:
            copy.wait()
        pltpu.make_async_copy(gate_ref, m_all.at[w_own], local_sem.at[5]).wait()
        pltpu.make_async_copy(up_ref, o_all.at[w_own], local_sem.at[6]).wait()
    with jax.named_scope("barrier"):
        pl.semaphore_wait(barrier, t + 2)

    def block_at(direction, back):
        return lax.rem(i + n - back, n) if direction == 0 else lax.rem(i + back, n)

    def turn(step, turns):
        return (step - 1) % turns if isinstance(step, int) else lax.rem(step - 1, turns)

    def kv_copy(direction, step, back, part):
        rows_of = pl.ds(0, tok) if part == 0 else pl.ds(tok, tok + LOGIT_ROWS)
        block = kv_all.at[block_at(direction, back), rows_of]
        return pltpu.make_async_remote_copy(
            src_ref=block,
            dst_ref=block,
            send_sem=kv_send.at[direction, part, turn(step, 2)],
            recv_sem=kv_recv.at[direction, part, turn(step, 8)],
            device_id={"sp": right if direction == 0 else left},
            device_id_type=MESH,
        )

    def half_of(direction, back, half):
        start = block_at(direction, back) * w_rows + half * half_rows
        return pl.ds(pl.multiple_of(start, half_rows), half_rows)

    quarter = half_rows // 2
    groups = first_steps // 4
    early = 3 * groups
    shared = max(0, early - BEHIND)

    def d_part(direction, back, part):
        if part == 0:
            return half_of(direction, back, 0)
        which = parity if part == 1 else 1 - parity
        start = block_at(direction, back) * w_rows + half_rows + which * quarter
        return pl.ds(pl.multiple_of(start, quarter), quarter)

    def w_copy(ref, send, recv, direction, step, half, rows_of):
        part = ref.at[rows_of]
        return pltpu.make_async_remote_copy(
            src_ref=part,
            dst_ref=part,
            send_sem=send,
            recv_sem=recv.at[direction, half, turn(step, 4)],
            device_id={"sp": right if direction == 0 else left},
            device_id_type=MESH,
        )

    def m_copy(direction, step, back, half):
        return w_copy(m_all, m_send, m_recv, direction, step, half, half_of(direction, back, half))

    def d_copy(direction, step, back, half):
        return w_copy(d_all, d_send, d_recv, direction, step, half, d_part(direction, back, half))

    def steps_of(direction, flipped):
        return first_steps if direction == int(flipped) else second_steps

    def if_step(condition, body):
        if isinstance(condition, bool):
            if condition:
                body()
        else:
            pl.when(condition)(body)

    def both(a, b):
        return (a and b) if isinstance(a, bool) else a & b

    def kv_moves(direction, step, back):
        if direction == 0:
            return (i >= back) & (i < n - 1) & (step <= first_steps)
        return (lax.rem(i + back, n) < second_steps) & (step <= second_steps)

    def kv_slot(s):
        for part in (0, 1):

            @pl.when((i >= s) & (s <= first_steps))
            def _(part=part):
                kv_copy(0, s, s, part).wait_recv()

            @pl.when(kv_moves(0, s + 1, s))
            def _(part=part):
                kv_copy(0, s + 1, s, part).start()

            @pl.when((lax.rem(i + s, n) < second_steps) & (s <= second_steps))
            def _(part=part):
                kv_copy(1, s, s, part).wait_recv()

            @pl.when(kv_moves(1, s + 1, s))
            def _(part=part):
                kv_copy(1, s + 1, s, part).start()

        for direction in (0, 1):

            @pl.when(kv_moves(direction, s, s - 1))
            def _(direction=direction):
                for part in (0, 1):
                    kv_copy(direction, s, s - 1, part).wait_send()

    def w_arrived(copy, s, half, direction, count):
        copy(direction, s, s, half).wait_recv()
        if_step(s < count, lambda: copy(direction, s + 1, s, half).start())

    def to_partner(src, dst, rows_of, send, recv):
        pltpu.make_async_remote_copy(
            src_ref=src.at[rows_of],
            dst_ref=dst.at[rows_of],
            send_sem=send,
            recv_sem=recv,
            device_id={"grp": partner},
            device_id_type=MESH,
        ).start()

    def wait_down(start, stop, which):
        blocks = min(stop - 1, first_steps) + min(stop - 1, second_steps)
        blocks -= min(start - 1, first_steps) + min(start - 1, second_steps)
        if blocks > 0:
            rest = d_all.at[pl.ds(0, blocks * quarter)]
            pltpu.make_async_copy(rest, rest, dy_recv.at[which]).wait()

    def d_first(half):
        for part in (1,) if half == 0 else (0, 2) if shared == 0 else (0,):
            for direction in (0, 1):
                d_copy(direction, 1, 0, part).start()

    def w_slot(s, half):
        d = s - BEHIND

        def m_parts():
            for direction in (0, 1):

                def m_arrived(direction=direction, count=steps_of(direction, True)):
                    w_arrived(m_copy, s, half, direction, count)
                    y_sem = y_recv.at[0 if not isinstance(s, int) or s <= early else 1]
                    to_partner(m_all, o_all, half_of(direction, s, half), y_send, y_sem)

                if_step(s <= steps_of(direction, True), m_arrived)
        def d_parts():
            if half == 0 and isinstance(d, int) and d == shared + 1 and shared > 0:
                wait_down(shared, shared + 1, 1)
                for direction in (0, 1):
                    if d <= steps_of(direction, False):
                        d_copy(direction, d, shared, 2).start()
            for part in (1,) if half == 0 else (0, 2):
                for direction in (0, 1):

                    def d_arrived(direction=direction, part=part, count=steps_of(direction, False)):
                        w_arrived(d_copy, d, part, direction, count)
                        if part == 1 and (not isinstance(d, int) or d <= shared):
                            dy_sem = dy_recv.at[int(d == shared) if isinstance(d, int) else (d == shared).astype(jnp.int32)]
                            to_partner(d_all, d_all, d_part(direction, d, 1), dy_send, dy_sem)

                    if part == 2 and not isinstance(d, int):
                        continue
                    if part == 2 and d <= shared:
                        continue
                    if_step(both(d > 0, d <= steps_of(direction, False)), d_arrived)

        for body in (d_parts, m_parts) if half == 0 else (m_parts, d_parts):
            body()

        if_step(s == BEHIND, lambda: d_first(half))

    for part in (0, 1):
        for direction in (0, 1):
            pl.when(kv_moves(direction, 1, 0))(kv_copy(direction, 1, 0, part).start)
    for half in (0, 1):
        for direction in (0, 1):
            m_copy(direction, 1, 0, half).start()
        if BEHIND == 0:
            d_first(half)

    def ow_block(index):
        return ow_all.at[pl.ds(pl.multiple_of(index * width, width), width)]

    def ow_copy(index, where, send, recv):
        return pltpu.make_async_remote_copy(
            src_ref=ow_block(index),
            dst_ref=ow_block(index),
            send_sem=send,
            recv_sem=recv,
            device_id={"tp": where},
            device_id_type=MESH,
        )

    for k in range(2, t, 2):
        ow_copy(c, peer(k), ow_send, ow_recv).start()
    ow_copy(c, sibling, ow_pass_send, ow_pass_recv).start()

    def ow_pass():
        x_rows = ow_all.at[pl.ds(0, (t // 2 - 1) * width)]
        pltpu.make_async_copy(x_rows, x_rows, ow_recv).wait()
        for k in range(2, t, 2):
            ow_copy(peer(k), sibling, ow_pass_send, ow_pass_recv).start()

    scale = width ** (-0.5)

    def terms(block, causal):
        k = kv_all[block, pl.ds(0, tok), :]
        v = kv_all[block, pl.ds(tok, tok), :]
        logit = kv_all[block, pl.ds(2 * tok, LOGIT_ROWS), :].astype(F32)[0:1, :]
        scores = lax.dot_general(
            q_ref[...], k, (((1,), (1,)), ((), ())), preferred_element_type=F32
        )
        scores = scores * scale + logit
        soft = jnp.log1p(jnp.exp(-jnp.abs(scores)))
        keep = -(jnp.maximum(scores, 0.0) + soft)
        if causal is not None:
            keep = jnp.where(causal, keep, 0.0)
        high = keep.astype(BF16)
        low = (keep - high.astype(F32)).astype(BF16)
        u = upper[...]
        sums = jnp.dot(high, u, preferred_element_type=F32) + jnp.dot(
            low, u, preferred_element_type=F32
        )
        within, total = sums[:, :tile], sums[:, tile:]
        stick = jnp.exp(jnp.minimum(scores, 0.0) - soft + within)
        if causal is not None:
            stick = jnp.where(causal, stick, 0.0)
        part = jnp.dot(stick.astype(BF16), v, preferred_element_type=F32)
        return total, part

    def attend_near(s):
        @pl.when(i >= s)
        def _():
            total, part = terms(i - s, None)
            so_far = run_near[...]
            acc_near[...] += jnp.exp(so_far) * part
            run_near[...] = so_far + total

    def attend_far(s):
        @pl.when((i + s >= n) & (s <= second_steps))
        def _():
            total, part = terms(i + s - n, None)
            acc_far[...] = acc_far[...] * jnp.exp(total) + part

    q_pos = lax.broadcasted_iota(jnp.int32, (tok, tok), 0)
    k_pos = lax.broadcasted_iota(jnp.int32, (tok, tok), 1)
    total, part = terms(i, k_pos < q_pos)
    acc_near[...] = part
    run_near[...] = total

    def group(g, carry):
        s, w = 4 * g, 3 * g
        if t > 2:
            pl.when(g == groups - 1)(ow_pass)
        with jax.named_scope("kv1"):
            kv_slot(s + 1)
        attend_near(s + 1)
        with jax.named_scope("w1a"):
            w_slot(w + 1, 0)
        attend_far(s + 1)
        with jax.named_scope("w1b"):
            w_slot(w + 1, 1)
        with jax.named_scope("kv2"):
            kv_slot(s + 2)
        attend_near(s + 2)
        with jax.named_scope("w2a"):
            w_slot(w + 2, 0)
        attend_far(s + 2)
        with jax.named_scope("kv3"):
            kv_slot(s + 3)
        attend_near(s + 3)
        with jax.named_scope("w2b"):
            w_slot(w + 2, 1)
        attend_far(s + 3)
        with jax.named_scope("w3a"):
            w_slot(w + 3, 0)
        with jax.named_scope("kv4"):
            kv_slot(s + 4)
        attend_near(s + 4)
        with jax.named_scope("w3b"):
            w_slot(w + 3, 1)
        attend_far(s + 4)
        return carry

    lax.fori_loop(0, groups, group, 0)

    def columns(index, size):
        return pl.ds(pl.multiple_of(index * size, size), size)

    def send_attended():
        own = columns(c, width)
        att_all[:, own] = (acc_near[...] + jnp.exp(run_near[...]) * acc_far[...]).astype(BF16)
        for k in range(1, t):
            pltpu.make_async_remote_copy(
                src_ref=att_all.at[:, own],
                dst_ref=att_all.at[:, own],
                send_sem=att_send,
                recv_sem=att_recv,
                device_id={"tp": peer(k)},
                device_id_type=MESH,
            ).start()


    def wait_attended():
        others = att_all.at[:, pl.ds(0, (t - 1) * width)]
        pltpu.make_async_copy(others, others, att_recv).wait()
        passed = ow_all.at[pl.ds(0, (t // 2) * width)]
        pltpu.make_async_copy(passed, passed, ow_pass_recv).wait()

    def project(start, stop):
        def step(j, carry):
            at = columns(j, wide)
            mixed[:, at] = jnp.dot(
                att_all[...], ow_all[:, at], preferred_element_type=F32
            ).astype(BF16)
            return carry

        lax.fori_loop(start, stop, step, 0)

    def normalize(x):
        return x * lax.rsqrt(jnp.mean(x * x, axis=-1, keepdims=True) + EPSILON)

    chunk = CHUNK

    def norms(start, stop):
        def step(j, carry):
            at = columns(j, chunk)
            mid = (
                res_ref[at, :].astype(F32)
                + mix_gain_ref[...] * normalize(mixed[at, :].astype(F32))
            ).astype(BF16)
            middle[at, :] = mid
            normed[at, :] = (ffn_gain_ref[...] * normalize(mid.astype(F32))).astype(BF16)
            return carry

        lax.fori_loop(start, stop, step, 0)

    chunks, per_chunk = d_model // wide, wide // w_rows
    arrived_chunks = max(0, min(chunks, (2 * early + 2 - per_chunk) // per_chunk))
    first_chunk = (i + n - early + per_chunk - 1) // per_chunk

    def act_of(weights, act, start, stop):
        def step(j, carry):
            at = columns(lax.rem(first_chunk + j, chunks), wide)
            act[...] += jnp.dot(normed[:, at], weights[at, :], preferred_element_type=F32)
            return carry

        lax.fori_loop(start, stop, step, 0)

    def wait_other(start, stop, which):
        blocks = min(stop - 1, first_steps) + min(stop - 1, second_steps)
        blocks -= min(start - 1, first_steps) + min(start - 1, second_steps)
        if blocks:
            rest = o_all.at[pl.ds(0, blocks * w_rows)]
            pltpu.make_async_copy(rest, rest, y_recv.at[which]).wait()

    def hide():
        def step(j, carry):
            at = columns(j, chunk)
            a, b = m_act[at, :], o_act[at, :]
            gate = jnp.where(parity == 0, a, b)
            up = jnp.where(parity == 0, b, a)
            hidden[at, :] = (gate / (1.0 + jnp.exp(-gate)) * up).astype(BF16)
            return carry

        lax.fori_loop(0, tok // chunk, step, 0)

    count, chips = d_model // wide, t // 2
    half_of_rows = tok // 2
    core, chip = lax.rem(c, 2), c // 2

    def rows_at(start, size):
        return pl.ds(pl.multiple_of(start, own_rows), size)

    own_half = rows_at(core * half_of_rows, half_of_rows)
    other_half = rows_at((1 - core) * half_of_rows, half_of_rows)
    in_half = rows_at(chip * own_rows, own_rows)
    own = rows_at(core * half_of_rows + chip * own_rows, own_rows)

    def to_peer(src, dst, send, recv, where):
        pltpu.make_async_remote_copy(
            src_ref=src,
            dst_ref=dst,
            send_sem=send,
            recv_sem=recv,
            device_id={"tp": where},
            device_id_type=MESH,
        ).start()

    def await_all(ref, sem):
        pltpu.make_async_copy(ref, ref, sem).wait()

    whole_at = first_steps - BEHIND
    first_tiles = max(0, min(count, (2 * whole_at + 2 - per_chunk) // per_chunk))
    first_tile = (i + n - whole_at + per_chunk - 1) // per_chunk

    def partial(j, carry):
        p = lax.rem(first_tile + j, count)
        parts[p] = lax.dot_general(
            hidden[...],
            d_all[columns(p, wide), :],
            (((1,), (1,)), ((), ())),
            preferred_element_type=F32,
        ).astype(BF16)
        to_peer(parts.at[p, other_half], core_buf.at[p], cs_send, cs_recv.at[p], sibling)
        return carry

    def between_cores(j, carry):
        p = lax.rem(first_tile + j, count)
        await_all(core_buf.at[p], cs_recv.at[p])
        halves[p] = (parts[p, own_half, :].astype(F32) + core_buf[p].astype(F32)).astype(BF16)
        for far in range(1, chips):
            to = lax.rem(chip + far, chips)
            to_peer(
                halves.at[p, rows_at(to * own_rows, own_rows)],
                rs_buf.at[p, far - 1],
                rs_send,
                rs_recv.at[p],
                2 * to + core,
            )
        return carry

    def between_chips(j, carry):
        p = lax.rem(first_tile + j, count)
        total = halves[p, in_half, :].astype(F32)
        if chips > 1:
            await_all(rs_buf.at[p], rs_recv.at[p])
        for far in range(1, chips):
            total = total + rs_buf[p, far - 1].astype(F32)
        ffn[p, own, :] = total.astype(BF16)
        return p

    def chips_then_cores(j, carry):
        p = between_chips(j, carry)
        for far in range(1, chips):
            to = 2 * lax.rem(chip + far, chips) + core
            to_peer(ffn.at[p, own], ffn.at[p, own], ag_send, ag_recv.at[p], to)
        return carry

    def to_all(p):
        for far in range(1, t):
            to_peer(ffn.at[p, own], ffn.at[p, own], lg_send.at[p], lg_recv.at[p], peer(far))

    def chips_then_all(j, carry):
        to_all(between_chips(j, carry))
        return carry

    def last_partial(j):
        p = lax.rem(first_tile + j, count)
        k = j - (count - LAST)
        parts[p] = lax.dot_general(
            hidden[...],
            d_all[columns(p, wide), :],
            (((1,), (1,)), ((), ())),
            preferred_element_type=F32,
        ).astype(BF16)
        for far in range(1, t):
            to = peer(far)
            start = lax.rem(to, 2) * half_of_rows + to // 2 * own_rows
            to_peer(
                parts.at[p, rows_at(start, own_rows)],
                rs_last.at[k, far - 1],
                ls_send,
                ls_recv.at[k],
                to,
            )

    def last_total(j):
        p = lax.rem(first_tile + j, count)
        k = j - (count - LAST)
        await_all(rs_last.at[k], ls_recv.at[k])
        total = parts[p, own, :].astype(F32)
        for far in range(1, t):
            total = total + rs_last[k, far - 1].astype(F32)
        ffn[p, own, :] = total.astype(BF16)
        to_all(p)

    def to_other_core(j, carry):
        p = lax.rem(first_tile + j, count)
        if chips > 1:
            await_all(rs_buf.at[p], ag_recv.at[p])
        to_peer(ffn.at[p, own_half], ffn.at[p, own_half], cg_send, cg_recv.at[p], sibling)
        return carry

    def zero_acts():
        m_act[...] = jnp.zeros_like(m_act)
        o_act[...] = jnp.zeros_like(o_act)

    n_cols, n_rows = d_model // wide, tok // chunk
    some = arrived_chunks // 2

    def named(name, *bodies):
        def run():
            with jax.named_scope(name):
                for body in bodies:
                    body()

        return run

    tasks = [
        named("zero", zero_acts),
        named("project1", wait_attended, lambda: project(0, n_cols // 2)),
        named("project2", lambda: project(n_cols // 2, n_cols)),
        named("norms1", lambda: norms(0, n_rows // 2)),
        named("norms2", lambda: norms(n_rows // 2, n_rows)),
        named("mine1", lambda: act_of(m_all, m_act, 0, some)),
        named("mine2", lambda: act_of(m_all, m_act, some, arrived_chunks)),
        named(
            "other1",
            lambda: wait_other(1, early + 1, 0),
            lambda: act_of(o_all, o_act, 0, arrived_chunks),
        ),
    ]
    after = [
        named("mine3", lambda: act_of(m_all, m_act, arrived_chunks, chunks)),
        named(
            "other2",
            lambda: wait_other(early + 1, first_steps + 1, 1),
            lambda: act_of(o_all, o_act, arrived_chunks, chunks),
            hide,
            lambda: wait_down(1, shared, 0),
        ),
    ]
    stages = {"partial": partial, "cores": between_cores}
    reached = dict.fromkeys(stages, 0)
    reduced = count - LAST
    near = min(first_tiles, reduced)
    third = (near + 2) // 3
    two = min(2 * third, near)

    def up_to(name, stop):
        def body():
            if reached[name] < stop:
                lax.fori_loop(reached[name], stop, stages[name], 0)
                reached[name] = stop

        return named(name, body)

    after += [
        up_to("partial", third),
        up_to("partial", two),
        lambda: (up_to("partial", near)(), up_to("cores", third)()),
        up_to("cores", two),
    ]
    with jax.named_scope("send_attended"):
        send_attended()
    for s in range(early + 1, first_steps + BEHIND + 1):
        for half in (0, 1):
            with jax.named_scope("wl" if s <= first_steps else "dl"):
                w_slot(s, half)
            if s == first_steps and half == 1:
                while tasks:
                    tasks.pop(0)()
                tasks = after
            elif tasks:
                tasks.pop(0)()
    while tasks:
        tasks.pop(0)()
    up_to("partial", reduced)()
    with jax.named_scope("last_partial"):
        for j in range(reduced, count):
            last_partial(j)
    up_to("cores", reduced)()
    with jax.named_scope("chips"):
        lax.fori_loop(0, two, chips_then_cores, 0)
    with jax.named_scope("last_total"):
        for j in range(reduced, count):
            last_total(j)
    with jax.named_scope("chips_all"):
        lax.fori_loop(two, reduced, chips_then_all, 0)
    with jax.named_scope("back"):
        lax.fori_loop(0, two, to_other_core, 0)

    with jax.named_scope("gathered"):
        for j in range(count):
            p = lax.rem(first_tile + j, count)
            if j < two:
                await_all(core_buf.at[p], cg_recv.at[p])
            else:
                await_all(rs_last.at[0], lg_recv.at[p])

    def finish(j, carry):
        at = columns(j, chunk)
        x = jnp.concatenate([ffn[p, at, :] for p in range(count)], axis=1).astype(F32)
        out[at, :] = (
            middle[at, :].astype(F32) + out_gain_ref[...] * normalize(x)
        ).astype(BF16)
        pltpu.make_async_copy(out.at[at], out_ref.at[at], out_sem).start()
        return carry

    with jax.named_scope("finish"):
        lax.fori_loop(0, tok // chunk, finish, 0)

    def drain(ref, sem):
        pltpu.make_async_copy(ref, ref, sem).wait()

    ring = pl.ds(0, (n - 1) * w_rows)
    drain(m_all.at[ring], m_send)
    drain(m_all.at[ring], y_send)
    over_y = min(shared, first_steps) + min(shared, second_steps)
    d_rows = (n - 1) * w_rows - over_y * quarter
    drain(d_all.at[pl.ds(0, d_rows)], d_send)
    if over_y:
        drain(d_all.at[pl.ds(0, over_y * quarter)], dy_send)
    if t > 2:
        drain(ow_all.at[pl.ds(0, (t // 2 - 1) * width)], ow_send)
    drain(ow_all.at[pl.ds(0, (t // 2) * width)], ow_pass_send)
    drain(att_all.at[:, pl.ds(0, (t - 1) * width)], att_send)
    if reduced:
        drain(core_buf.at[pl.ds(0, reduced)], cs_send)
        if chips > 1:
            drain(rs_buf.at[pl.ds(0, reduced)], rs_send)
    if two:
        drain(core_buf.at[pl.ds(0, two)], cg_send)
        if chips > 1:
            drain(rs_buf.at[pl.ds(0, two)], ag_send)
    drain(rs_last, ls_send)
    for j in range(two, count):
        drain(rs_last.at[0], lg_send.at[lax.rem(first_tile + j, count)])
    pltpu.make_async_copy(out, out_ref, out_sem).wait()


def solution(mesh):
    n, t = mesh.shape["sp"], mesh.shape["tp"]

    def shards(
        query_rows,
        key_rows,
        value_rows,
        key_logit,
        residual,
        out_weight,
        mix_gain,
        ffn_gain,
        out_gain,
        gate_weight,
        up_weight,
        down_weight,
    ):
        tok, width = query_rows.shape
        w_rows, units = gate_weight.shape
        d_model = residual.shape[1]
        tile = 128
        count = d_model // WIDE
        logit = jnp.broadcast_to(key_logit.reshape(1, tok), (LOGIT_ROWS, tok))
        hbm = pl.BlockSpec(memory_space=pltpu.HBM)
        dma = pltpu.SemaphoreType.DMA
        return pl.pallas_call(
            functools.partial(layer_kernel, (n, t)),
            out_shape=jax.ShapeDtypeStruct((tok, d_model), BF16),
            in_specs=[hbm] * 12,
            out_specs=hbm,
            scratch_shapes=[
                pltpu.VMEM((tok, width), BF16),
                pltpu.VMEM((tok, d_model), BF16),
                pltpu.VMEM((1, d_model), F32),
                pltpu.VMEM((1, d_model), F32),
                pltpu.VMEM((1, d_model), F32),
                pltpu.VMEM((n, 2 * tok + LOGIT_ROWS, width), BF16),
                pltpu.VMEM((n * w_rows, units), BF16),
                pltpu.VMEM((n * w_rows, units), BF16),
                pltpu.VMEM((n * w_rows, units), BF16),
                pltpu.VMEM((t * width, d_model), BF16),
                pltpu.VMEM((tok, t * width), BF16),
                pltpu.VMEM((tok, d_model), BF16),
                pltpu.VMEM((tok, d_model), BF16),
                pltpu.VMEM((tok, d_model), BF16),
                pltpu.VMEM((tok, units), F32),
                pltpu.VMEM((tok, units), F32),
                pltpu.VMEM((tok, units), BF16),
                pltpu.VMEM((count, tok, WIDE), BF16),
                pltpu.VMEM((count, tok // 2, WIDE), BF16),
                pltpu.VMEM((count, tok // 2, WIDE), BF16),
                pltpu.VMEM((count, max(t // 2 - 1, 1), tok // t, WIDE), BF16),
                pltpu.VMEM((count, tok, WIDE), BF16),
                pltpu.VMEM((tile, 2 * tile), BF16),
                pltpu.VMEM((tok, width), F32),
                pltpu.VMEM((tok, width), F32),
                pltpu.VMEM((tok, width), F32),
                dma((12,)),
                dma((2, 2, 2)),
                dma((2, 2, 8)),
                dma,
                dma((2, 2, 4)),
                dma,
                dma((2, 3, 4)),
                dma,
                dma((2,)),
                dma,
                dma,
                dma,
                dma,
                dma,
                dma,
                dma,
                dma((count,)),
                dma,
                dma((count,)),
                dma,
                dma((count,)),
                dma,
                dma((count,)),
                dma,
                dma((2,)),
                pltpu.VMEM((tok, d_model), BF16),
                dma,
                pltpu.VMEM((LAST, t - 1, tok // t, WIDE), BF16),
                dma,
                dma((LAST,)),
                dma((count,)),
                dma((count,)),
            ],
            compiler_params=pltpu.CompilerParams(
                collective_id=0, has_side_effects=True, vmem_limit_bytes=67043328
            ),
            name="layer",
        )(
            query_rows,
            key_rows,
            value_rows,
            logit,
            residual,
            out_weight,
            mix_gain.reshape(1, d_model),
            ffn_gain.reshape(1, d_model),
            out_gain.reshape(1, d_model),
            gate_weight,
            up_weight,
            down_weight,
        )

    rows = P(("grp", "sp"), "tp")
    placed = (
        rows,
        rows,
        rows,
        rows,
        P(("grp", "sp"), None),
        P("tp", None),
        P(),
        P(),
        P(),
        P("sp", "tp"),
        P("sp", "tp"),
        P("sp", "tp"),
    )
    return jax.shard_map(
        shards, mesh=mesh, in_specs=placed, out_specs=P(("grp", "sp"), None), check_vma=False
    )
```
